512 devices in a mesh: kv: 64 (over z, y), tp: 8 (over x, core).
Axes of the slice: x: 4, y: 8, z: 8, core: 2. Of those that a mesh axis runs over, the one named last changes fastest.
Arguments:
- tokens: bfloat16 [256, 2048], P('tp', 'kv'), may hold values from -60 to 60
- gain_mix: float32 [2048], P('kv'), may hold values from 0.1 to 1.9
- w_query: bfloat16 [2048, 2048], P('kv', 'tp'), may hold values from -0.125 to 0.125
- w_key: bfloat16 [2048, 2048], P('kv', 'tp'), may hold values from -0.125 to 0.125
- w_value: bfloat16 [2048, 2048], P('kv', 'tp'), may hold values from -0.125 to 0.125
- w_igate: bfloat16 [2048, 8], P('kv', 'tp'), may hold values from -0.125 to 0.125
- w_fgate: bfloat16 [2048, 8], P('kv', 'tp'), may hold values from -0.125 to 0.125
- bias_igate: float32 [8], P('tp'), may hold values from -3 to 3
- bias_fgate: float32 [8], P('tp'), may hold values from -3 to 3
- state_mem: float32 [256, 8, 256, 256], P('kv', 'tp'), may hold values from -2 to 2
- state_max: float32 [256, 8], P('kv', 'tp'), may hold values from -60 to 220
- keys_blk: bfloat16 [256, 8, 128, 256], P('kv', 'tp'), may hold values from -6 to 6
- values_blk: bfloat16 [256, 8, 128, 256], P('kv', 'tp'), may hold values from -6 to 6
- igate_blk: float32 [256, 8, 128], P('kv', 'tp'), may hold values from -10 to 220
- fgate_blk: float32 [256, 8, 128], P('kv', 'tp'), may hold values from -3 to 0
- lengths: int32 [256], P('kv'), may hold values from 1 to 127, 8192 in all
- gain_head: float32 [256], replicated, may hold values from 0.1 to 1.9
- w_mixout: bfloat16 [2048, 2048], P('tp', 'kv'), may hold values from -0.25 to 0.25
- gain_mlp: float32 [2048], P('kv'), may hold values from 0.1 to 1.9
- w_up: bfloat16 [2048, 8192], P('kv', 'tp'), may hold values from -0.125 to 0.125
- w_down: bfloat16 [8192, 2048], P('tp', 'kv'), may hold values from -0.0625 to 0.0625
Outputs:
- layer_out: bfloat16 [256, 2048], P('tp', 'kv')
The draws below stay inside these ranges and needn't reach their ends.
Inputs may be any that keep to these rules, and one draw needn't show every extreme that they name: `lengths`: entries of a sequence's block at or past its length are not live. The largest length is reached in every draw.
All inputs are finite; a program needn't handle non-finite values.
Results may differ from the reference program's by a relative error of at most 0.015.
Values may be sent and summed in bfloat16 or wider, within the bound.
A program may use at most 64 MiB of HBM per device.

```python
import math
import jax
import jax.numpy as jnp
import numpy as np
from jax import lax

D = 2048
CELL_FACETS = 8
HD = 256
FF = 8192
SEGMENT_LENGTH = 128
STREAM_TOTAL = 256
D_ML = 2048
N_TP = 8


def draw_tokens(key, part):
    addressing_arrays = jax.random.split(key, 1)
    base = jax.random.normal(addressing_arrays[0], (STREAM_TOTAL, D), jnp.float32)
    columns = jnp.exp(jnp.log(0.4) + jnp.log(10.0) * jnp.arange(D, dtype=jnp.float32) / (D - 1))
    values = jnp.clip(base, -6.0, 6.0)
    return jnp.clip(values * columns[None, :], -60.0, 60.0).astype(jnp.bfloat16)


def draw_state_max(key, part):
    return jax.random.uniform(key, (STREAM_TOTAL, CELL_FACETS), jnp.float32, -1.0, 2.0)


def draw_igate_blk(key, part):
    addressing_arrays = jax.random.split(key, 1)
    return jnp.clip(jax.random.normal(addressing_arrays[0], (STREAM_TOTAL, CELL_FACETS, SEGMENT_LENGTH), jnp.float32), -6.0, 6.0)


def draw_fgate_blk(key, part):
    addressing_arrays = jax.random.split(key, 7)
    share = 0.5
    quick = jax.random.bernoulli(addressing_arrays[0], share, (STREAM_TOTAL, CELL_FACETS, 1))
    quick_rate = jax.random.uniform(addressing_arrays[1], (STREAM_TOTAL, CELL_FACETS, 1), jnp.float32, 2.0, 4.0) / 40.0
    slow_rate = jax.random.uniform(addressing_arrays[2], (STREAM_TOTAL, CELL_FACETS, 1), jnp.float32, 0.1, 0.8) / SEGMENT_LENGTH
    seqfactor = jnp.exp(jax.random.uniform(addressing_arrays[3], (STREAM_TOTAL, 1, 1), jnp.float32, jnp.log(0.5), jnp.log(2.0)))
    shrinking_quotient = jnp.where(quick, quick_rate, slow_rate) * seqfactor
    arbitrary_shift = jax.random.uniform(addressing_arrays[4], (STREAM_TOTAL, CELL_FACETS, SEGMENT_LENGTH), jnp.float32, 0.5, 1.5)
    segment_clusters = jax.random.bernoulli(addressing_arrays[5], 3.0 / SEGMENT_LENGTH, (STREAM_TOTAL, CELL_FACETS, SEGMENT_LENGTH))
    training_loss = jnp.log(jax.random.uniform(addressing_arrays[6], (STREAM_TOTAL, CELL_FACETS, SEGMENT_LENGTH), jnp.float32, 0.5, 0.8))
    return -shrinking_quotient * arbitrary_shift + jnp.where(segment_clusters, training_loss, 0.0)


def level_of(own_key, dims, cuts, least, high):
    gain, own = 1.0, jax.random.fold_in(own_key, 6)
    for position, blocks in cuts:
        draws = jnp.exp(jax.random.uniform(jax.random.fold_in(own, position), (blocks,), jnp.float32, least / len(cuts), high / len(cuts)))
        gain = gain * jnp.repeat(draws, dims[position] // blocks).reshape([-1 if axis == position else 1 for axis in range(len(dims))])
    return gain


def split_up(count, total, most, skew):
    portions = [(1 << 20) // math.isqrt(standing ** skew) + 1 for standing in range(2, count + 1)]
    rest, holding = total - most - (count - 1), [1] * (count - 1)
    while rest > 0:
        candidates = [i for i in range(count - 1) if holding[i] < most]
        whole, budget = sum([portions[i] for i in candidates]), rest
        for i in candidates:
            extra = min(most - holding[i], max(1, budget * portions[i] // whole), rest)
            holding[i] = holding[i] + extra
            rest = rest - extra
    return np.array([most] + holding)


def ragged(rng, amount, total, reach, lean):
    if amount == 2:
        one = jax.random.randint(rng, (), max(1, total - reach), min(reach, total - 1) + 1)
        return jnp.stack([one, total - one])
    sizes = jnp.asarray(split_up(amount, total, reach, lean), jnp.int32)
    couples = (amount - 1) // 2
    giver, sink = sizes[1:1 + 2 * couples:2], sizes[2:2 + 2 * couples:2]
    room = jnp.minimum(giver - 1, reach - sink)
    moved = jax.random.randint(jax.random.fold_in(rng, 1), (couples,), 0, 1 << 20) % (room + 1)
    sizes = sizes.at[1:1 + 2 * couples:2].set(giver - moved).at[2:2 + 2 * couples:2].set(sink + moved)
    return sizes[jax.random.permutation(jax.random.fold_in(rng, 2), amount)]


def noise(own_key, dims, width, limit, shards=(), kind=jnp.bfloat16):
    entries = jax.random.normal(own_key, dims, jnp.float32) * width
    if len(shards) > 0:
        entries = level_of(own_key, dims, shards, -0.22, 0.18) * entries
    return jnp.clip(entries, min=-limit, max=limit).astype(kind)


def setup_inputs(seed: int = 0) -> dict:
    key_of = jax.random.split(jax.random.key(seed), 22)
    return {
        "tokens": draw_tokens(jax.random.fold_in(key_of[21], 71), 0),
        "gain_mix": jnp.clip(1.0 + 0.18 * jax.random.normal(key_of[1], (D,), jnp.float32), 0.1, 1.9),
        "w_query": noise(key_of[2], (D, D_ML), D ** -0.5, 0.125, ((0, 64), (1, 8))),
        "w_key": noise(key_of[3], (D, D_ML), D ** -0.5, 0.125, ((0, 64), (1, 8))),
        "w_value": noise(key_of[4], (D, D_ML), D ** -0.5, 0.125, ((0, 64), (1, 8))),
        "w_igate": noise(key_of[5], (D, CELL_FACETS), D ** -0.5, 0.125, ((0, 64), (1, 8))),
        "w_fgate": noise(key_of[6], (D, CELL_FACETS), D ** -0.5, 0.125, ((0, 64), (1, 8))),
        "bias_igate": noise(key_of[7], (CELL_FACETS,), 1.0, 3.0, ((0, 8),), jnp.float32),
        "bias_fgate": noise(key_of[8], (CELL_FACETS,), 1.0, 3.0, ((0, 8),), jnp.float32),
        "state_mem": noise(key_of[9], (STREAM_TOTAL, CELL_FACETS, HD, HD), 0.3, 2.0, ((0, 64), (1, 8)), jnp.float32),
        "state_max": draw_state_max(jax.random.fold_in(key_of[21], 71), 0),
        "keys_blk": noise(key_of[11], (STREAM_TOTAL, CELL_FACETS, SEGMENT_LENGTH, HD), 1.0, 6.0, ((0, 64), (1, 8))),
        "values_blk": noise(key_of[12], (STREAM_TOTAL, CELL_FACETS, SEGMENT_LENGTH, HD), 1.0, 6.0, ((0, 64), (1, 8))),
        "igate_blk": draw_igate_blk(jax.random.fold_in(key_of[21], 71), 0),
        "fgate_blk": draw_fgate_blk(jax.random.fold_in(key_of[21], 71), 0),
        "lengths": ragged(key_of[15], STREAM_TOTAL, STREAM_TOTAL * SEGMENT_LENGTH // 4, SEGMENT_LENGTH - 1, 2).astype(jnp.int32),
        "gain_head": jnp.clip(1.0 + 0.18 * jax.random.normal(key_of[16], (HD,), jnp.float32), 0.1, 1.9),
        "w_mixout": noise(key_of[17], (D_ML, D), (D_ML // 4) ** -0.5, 0.25, ((0, 8), (1, 64))),
        "gain_mlp": jnp.clip(1.0 + 0.18 * jax.random.normal(key_of[18], (D,), jnp.float32), 0.1, 1.9),
        "w_up": noise(key_of[19], (D, FF), D ** -0.5, 0.125, ((0, 64), (1, 8))),
        "w_down": noise(key_of[20], (FF, D), FF ** -0.5, 0.0625, ((0, 8), (1, 64))),
    }


EPS = 1e-06

def rms_factor(values):
    return lax.rsqrt(lax.optimization_barrier(jnp.mean(values * values, axis=-1, keepdims=True)) + EPS)

def memory_cell(query, key_new, value_new, input_gate, forget_gate, state_mem, state_max, keys_blk, values_blk, igate_blk, fgate_blk, lengths, gain_head):
    span = keys_blk.shape[2]
    head_size = query.shape[-1]
    positions = jnp.arange(span, dtype=jnp.int32)
    live_mask = positions[None, None, :] < lengths.astype(jnp.int32)[:, None, None]
    forget_live = jnp.where(live_mask, fgate_blk, 0.0)
    cumulative = jnp.cumsum(forget_live, axis=-1)
    total = cumulative[..., -1]
    suffix = total[..., None] - cumulative + forget_gate[..., None]
    past = igate_blk + suffix
    carried = state_max + total + forget_gate
    topmost = jnp.maximum(jnp.maximum(carried, input_gate), lax.optimization_barrier(jnp.max(jnp.where(live_mask, past, -jnp.inf), axis=-1)))
    scale = head_size ** (-0.5)
    query_f = query.astype(jnp.float32)
    scores = jnp.einsum('bhd,bhsd->bhs', query_f, keys_blk.astype(jnp.float32)) * scale
    weights = (jnp.where(live_mask, jnp.exp(past - topmost[..., None]), 0.0) * scores).astype(jnp.bfloat16)
    block_term = jnp.einsum('bhs,bhsd->bhd', weights.astype(jnp.float32), values_blk.astype(jnp.float32))
    state_term = jnp.einsum('bhvk,bhk->bhv', state_mem, query_f, precision=lax.Precision.HIGHEST) * jnp.exp(carried - topmost)[..., None]
    own_score = lax.optimization_barrier(jnp.sum(query_f * key_new.astype(jnp.float32), axis=-1)) * scale
    own_term = (jnp.exp(input_gate - topmost) * own_score)[..., None] * value_new.astype(jnp.float32)
    numerator = state_term + block_term + own_term
    normed = numerator * rms_factor(numerator) * gain_head
    return normed.astype(jnp.bfloat16).reshape(query.shape[0], -1)

def grouped_sum(left, right):
    left_groups = left.reshape(left.shape[0], N_TP, -1).astype(jnp.float32)
    right_groups = right.reshape(N_TP, -1, right.shape[1]).astype(jnp.float32)
    partials = jnp.einsum('bgc,gcd->gbd', left_groups, right_groups)
    rounded = lax.optimization_barrier(partials.astype(jnp.bfloat16))
    return lax.optimization_barrier(jnp.sum(rounded.astype(jnp.float32), axis=0))

def reference(tokens, gain_mix, w_query, w_key, w_value, w_igate, w_fgate, bias_igate, bias_fgate, state_mem, state_max, keys_blk, values_blk, igate_blk, fgate_blk, lengths, gain_head, w_mixout, gain_mlp, w_up, w_down):
    widened = tokens.astype(jnp.float32)
    factor_in = rms_factor(widened)
    scaled_in = (widened * gain_mix).astype(jnp.bfloat16)

    def project(weight):
        return jnp.dot(scaled_in, weight, preferred_element_type=jnp.float32) * factor_in
    query = project(w_query).astype(jnp.bfloat16).reshape(STREAM_TOTAL, CELL_FACETS, HD)
    key_new = project(w_key).astype(jnp.bfloat16).reshape(STREAM_TOTAL, CELL_FACETS, HD)
    value_new = project(w_value).astype(jnp.bfloat16).reshape(STREAM_TOTAL, CELL_FACETS, HD)
    input_gate = project(w_igate) + bias_igate
    forget_gate = jax.nn.log_sigmoid(project(w_fgate) + bias_fgate)
    mixed = memory_cell(query, key_new, value_new, input_gate, forget_gate, state_mem, state_max, keys_blk, values_blk, igate_blk, fgate_blk, lengths, gain_head)
    attended = grouped_sum(mixed, w_mixout)
    residual = (widened + attended).astype(jnp.bfloat16)
    restored = residual.astype(jnp.float32)
    factor_mid = rms_factor(restored)
    scaled_mid = (restored * gain_mlp).astype(jnp.bfloat16)
    upward = jnp.dot(scaled_mid, w_up, preferred_element_type=jnp.float32) * factor_mid
    hidden = jnp.square(jax.nn.relu(upward)).astype(jnp.bfloat16)
    return (restored + grouped_sum(hidden, w_down)).astype(jnp.bfloat16)
```

```python
import jax
import jax.numpy as jnp
from jax import lax
from jax.experimental import pallas as pl
from jax.experimental.pallas import tpu as pltpu
from jax.sharding import PartitionSpec as P

MESH = pl.DeviceIdType.MESH
F32, BF16 = jnp.float32, jnp.bfloat16
D = 2048
EPS = 1e-06
SCALE = 256 ** (-0.5)


def at_lanes(rows, offset, width):
    lane = lax.broadcasted_iota(jnp.int32, (rows, width), 1)
    row = lax.broadcasted_iota(jnp.int32, (rows, width), 0)
    return jnp.where(lane == row + offset, 1.0, 0.0)


def contract_last(a, b):
    return lax.dot_general(a, b, (((1,), (1,)), ((), ())), preferred_element_type=F32)


def column(row_ref, rows):
    n = row_ref.shape[1]
    v = jnp.broadcast_to(row_ref[...].astype(F32), (rows, n))
    lane = lax.broadcasted_iota(jnp.int32, (rows, n), 1)
    row = lax.broadcasted_iota(jnp.int32, (rows, n), 0)
    return jnp.sum(jnp.where(lane == row, v, 0.0), axis=1, keepdims=True)


def kernel(
    tok_h, gmix_h, wq_h, wk_h, wv_h, wi_h, wf_h, bi_h, bf_h, st_h, smax_h, k_h, v_h, ig_h, fg_h, len_h, gh_h, wm_h, gm_h,
    wu_h, wd_h, out_ref,
    tok, gmix, wi, wf, bi, bfg, st, smax, kb, vb, igb, fgb, lens, gh, gm,
    w1g, w2g, wmg, wug, wdg,
    ma, ra, a2, sb, rb, xraw, xsc, mz1, rz1, mz2, rz2, slo, shi, rows8, q16, w16, mc, rc, m32, md, rd, res, mf, rf, mg, rg, h32,
    mh, rh, mi, ri,
    lsem, ssem, rsem,
):
    kv = lax.axis_index("kv")
    t = lax.axis_index("tp")
    z = lax.shift_right_logical(kv, 3)
    y = lax.bitwise_and(kv, 7)
    zs = lambda i: (lax.bitwise_xor(kv, 8 * i), t)
    ys = lambda i: (lax.bitwise_xor(kv, i), t)
    ts = lambda i: (kv, lax.bitwise_xor(t, i))

    barrier = pltpu.get_barrier_semaphore()
    for who in (ys, ts, zs):
        for i in range(1, 8):
            pl.semaphore_signal(barrier, inc=1, device_id=who(i), device_id_type=MESH)

    loads = []

    def load(src, dst):
        c = pltpu.make_async_copy(src, dst, lsem.at[len(loads)])
        c.start()
        loads.append(c)
        return c

    l_tok = load(tok_h, tok)
    l_gmix = load(gmix_h, gmix)
    l_wi = load(wi_h, wi)
    l_wf = load(wf_h, wf)
    l_gm = load(gm_h, gm)
    l_w1 = load(wq_h, w1g.at[y])
    l_wk = load(wk_h, w2g.at[y, :, pl.ds(0, 256)])
    l_wv = load(wv_h, w2g.at[y, :, pl.ds(256, 256)])
    l_wm = load(wm_h, wmg.at[y])
    l_wu = load(wu_h, wug.at[y])
    l_wd = load(wd_h, wdg.at[y])
    cell = [
        load(a, b)
        for a, b in (
            (st_h, st), (smax_h, smax), (k_h, kb), (v_h, vb), (ig_h, igb), (fg_h, fgb), (len_h, lens), (gh_h, gh),
            (bi_h, bi), (bf_h, bfg),
        )
    ]

    pending = []

    def send(n, src, dst, who):
        for i in range(1, 8):
            c = pltpu.make_async_remote_copy(
                src_ref=src(i), dst_ref=dst, send_sem=ssem.at[n], recv_sem=rsem.at[n], device_id=who(i), device_id_type=MESH
            )
            c.start()
        pending.append((n, dst))

    def arrive(n, buf):
        part = buf.at[pl.ds(0, 7)]
        pltpu.make_async_copy(part, part, rsem.at[n]).wait()

    def left(n, buf):
        part = buf.at[pl.ds(0, 7)]
        pltpu.make_async_copy(part, part, ssem.at[n]).wait()

    place = at_lanes(32, 32 * y, 256)
    place_b = place.astype(BF16)
    l_tok.wait()
    l_gmix.wait()
    raw = tok[...].astype(F32)
    scaled = (raw * gmix[...]).astype(BF16)
    raw_p = jnp.dot(tok[...], place_b, preferred_element_type=F32)
    sc_p = jnp.dot(scaled, place_b, preferred_element_type=F32)
    for j in range(8):
        both = jnp.concatenate([raw_p[4 * j : 4 * j + 4], sc_p[4 * j : 4 * j + 4]], axis=0)
        ma[j] = both.astype(BF16)
    ra[y] = ma[y]

    l_wi.wait()
    l_wf.wait()
    l_gm.wait()
    g0 = gm[...]
    g1 = g0.astype(BF16).astype(F32)
    g2 = (g0 - g1).astype(BF16).astype(F32)
    g3 = g0 - g1 - g2
    row8 = lax.broadcasted_iota(jnp.int32, (8, 32), 0)
    six = jnp.zeros((8, 32), F32)
    for r, v in enumerate((wi[...].astype(F32), wf[...].astype(F32), g1, g2, g3)):
        six = jnp.where(row8 == r, jnp.broadcast_to(v, (8, 32)), six)
    a2[y] = jnp.dot(six.astype(BF16), place_b, preferred_element_type=F32).astype(BF16)

    l_w1.wait()
    l_wk.wait()
    l_wv.wait()
    pl.semaphore_wait(barrier, 21)

    send(0, lambda i: ma.at[lax.bitwise_xor(y, i)], ra.at[y], ys)
    send(1, lambda i: a2.at[y], a2.at[y], ys)
    send(2, lambda i: w1g.at[y], w1g.at[y], ys)
    send(3, lambda i: w2g.at[y], w2g.at[y], ys)

    for c in cell:
        c.wait()
    for s in range(4):
        hi = st[s, 0].astype(BF16)
        shi[s] = hi
        slo[s] = (st[s, 0] - hi.astype(F32)).astype(BF16)
    rows8[...] = jnp.zeros(rows8.shape, F32)
    for s in range(4):
        rows8[0, s : s + 1, :] = igb[s]
        rows8[1, s : s + 1, :] = fgb[s]
    lane = lax.broadcasted_iota(jnp.int32, (8, 128), 1)
    row = lax.broadcasted_iota(jnp.int32, (8, 128), 0)
    live = lane.astype(F32) < column(lens, 8)
    forget_live = jnp.where(live, rows8[1], 0.0)
    total = jnp.sum(forget_live, axis=1, keepdims=True)
    after = jnp.where(
        lax.broadcasted_iota(jnp.int32, (128, 128), 0) > lax.broadcasted_iota(jnp.int32, (128, 128), 1), 1.0, 0.0
    )
    past0 = rows8[0] + jnp.dot(forget_live, after, precision=lax.Precision.HIGHEST, preferred_element_type=F32)
    past0_top = jnp.max(jnp.where(live, past0, -1e30), axis=1, keepdims=True)
    carried0 = column(smax, 8) + total
    q16[...] = jnp.zeros(q16.shape, F32)
    w16[...] = jnp.zeros(w16.shape, F32)

    arrive(0, ra)
    joined = ra[0].astype(F32)
    for j in range(1, 8):
        joined += ra[j].astype(F32)
    sb[...] = joined.astype(BF16)
    rb[t] = joined.astype(BF16)
    send(4, lambda i: sb, rb.at[t], ts)
    l_wm.wait()
    send(5, lambda i: wmg.at[y], wmg.at[y], ys)

    arrive(4, rb)
    squares = []
    for j in range(8):
        b = rb[j].astype(F32)
        xraw[4 * j : 4 * j + 4, :] = b[0:4]
        xsc[4 * j : 4 * j + 4, :] = b[4:8]
    square_in = jnp.sum(xraw[...] * xraw[...], axis=1, keepdims=True)
    x = xsc[...].astype(BF16)
    arrive(1, a2)
    small = a2[0].astype(F32)
    for j in range(1, 8):
        small += a2[j].astype(F32)
    wgates = jnp.concatenate([small, jnp.zeros((120, 256), F32)], axis=0).astype(BF16)
    gain_mid = small[2:3] + small[3:4] + small[4:5]
    lane32 = lax.broadcasted_iota(jnp.int32, (32, 128), 1)

    def with_square(block, sq, at):
        hi = sq.astype(BF16).astype(F32)
        return jnp.where(lane32 == at, hi, jnp.where(lane32 == at + 1, sq - hi, block))

    gates = with_square(contract_last(x, wgates), square_in, 2)
    arrive(2, w1g)
    q_part = jnp.dot(x, w1g[...].reshape(256, 256), preferred_element_type=F32)
    for j in range(8):
        mz1[j, :, 0:256] = q_part[4 * j : 4 * j + 4].astype(BF16)
        mz1[j, :, 256:384] = gates[4 * j : 4 * j + 4].astype(BF16)
    rz1[z] = mz1[z]
    send(6, lambda i: mz1.at[lax.bitwise_xor(z, i)], rz1.at[z], zs)
    l_wu.wait()
    send(7, lambda i: wug.at[y], wug.at[y], ys)
    arrive(3, w2g)
    kv_part = jnp.dot(x, w2g[...].reshape(256, 512), preferred_element_type=F32)
    for j in range(8):
        mz2[j] = kv_part[4 * j : 4 * j + 4].astype(BF16)
    rz2[z] = mz2[z]
    send(8, lambda i: mz2.at[lax.bitwise_xor(z, i)], rz2.at[z], zs)
    l_wd.wait()
    send(9, lambda i: wdg.at[y], wdg.at[y], ys)

    arrive(6, rz1)
    first = rz1[0].astype(F32)
    for j in range(1, 8):
        first += rz1[j].astype(F32)
    own = first[:, 256:384]
    factor = lax.rsqrt((own[:, 2:3] + own[:, 3:4]) / D + EPS)
    q16[0:4, :] = first[:, 0:256] * factor
    rows8[2, 0:4, :] = own * factor
    gate8 = rows8[2]
    input_gate = gate8[:, 0:1] + bi[...]
    pre = gate8[:, 1:2] + bfg[...]
    forget_gate = jnp.minimum(pre, 0.0) - jnp.log1p(jnp.exp(-jnp.abs(pre)))
    carried = carried0 + forget_gate
    topmost = jnp.maximum(jnp.maximum(carried, input_gate), past0_top + forget_gate)
    decay = jnp.where(live, jnp.exp(jnp.minimum(past0 + forget_gate - topmost, 0.0)), 0.0)
    qb = q16[...].astype(BF16)
    scores = jnp.zeros((8, 128), F32)
    state = jnp.zeros((8, 256), F32)
    row256 = lax.broadcasted_iota(jnp.int32, (8, 256), 0)
    for s in range(4):
        scores = jnp.where(row == s, contract_last(qb, kb[s, 0])[0:8], scores)
        part = contract_last(qb, shi[s])[0:8] + contract_last(qb, slo[s])[0:8]
        state = jnp.where(row256 == s, part, state)
    w16[0:8, :] = decay * (scores * SCALE)
    wb = w16[...].astype(BF16)
    block = jnp.zeros((8, 256), F32)
    for s in range(4):
        block = jnp.where(row256 == s, jnp.dot(wb, vb[s, 0], preferred_element_type=F32)[0:8], block)
    numerator = jnp.exp(carried - topmost) * state + block
    own_scale = jnp.exp(input_gate - topmost) * SCALE

    arrive(8, rz2)
    second = rz2[0].astype(F32)
    for j in range(1, 8):
        second += rz2[j].astype(F32)
    second = (second * factor).astype(BF16).astype(F32)
    own_score = jnp.sum(qb[0:4].astype(F32) * second[:, 0:256], axis=1, keepdims=True)
    num = numerator[0:4] + (own_scale[0:4] * own_score) * second[:, 256:512]
    mixed = num * lax.rsqrt(jnp.mean(num * num, axis=1, keepdims=True) + EPS) * gh[...]
    mc[...] = mixed.astype(BF16)
    rc[z] = mixed.astype(BF16)
    send(10, lambda i: mc, rc.at[z], zs)

    arrive(5, wmg)
    arrive(10, rc)
    for j in range(8):
        m32[4 * j : 4 * j + 4, :] = rc[j].astype(F32)
    att = contract_last(m32[...].astype(BF16), wmg[...].reshape(256, 256)).astype(BF16)
    md[...] = att
    rd[t] = att
    send(11, lambda i: md, rd.at[t], ts)
    arrive(11, rd)
    attended = rd[0].astype(F32)
    for j in range(1, 8):
        attended += rd[j].astype(F32)
    restored = (xraw[...] + attended).astype(BF16).astype(F32)
    for j in range(8):
        res[j] = restored[4 * j : 4 * j + 4]

    square_mid = jnp.sum(restored * restored, axis=1, keepdims=True)
    sq_block = with_square(jnp.zeros((32, 128), F32), square_mid, 0)
    arrive(7, wug)
    up = jnp.dot((restored * gain_mid).astype(BF16), wug[...].reshape(256, 1024), preferred_element_type=F32)
    for j in range(8):
        mf[j, :, 0:1024] = up[4 * j : 4 * j + 4].astype(BF16)
        mf[j, :, 1024:1152] = sq_block[4 * j : 4 * j + 4].astype(BF16)
    rf[z] = mf[z]
    send(12, lambda i: mf.at[lax.bitwise_xor(z, i)], rf.at[z], zs)
    arrive(12, rf)
    whole = rf[0].astype(F32)
    for j in range(1, 8):
        whole += rf[j].astype(F32)
    factor_mid = lax.rsqrt((whole[:, 1024:1025] + whole[:, 1025:1026]) / D + EPS)
    hid = jnp.square(jnp.maximum(whole[:, 0:1024] * factor_mid, 0.0)).astype(BF16)
    mg[...] = hid
    rg[z] = hid
    send(13, lambda i: mg, rg.at[z], zs)

    arrive(9, wdg)
    arrive(13, rg)
    for j in range(8):
        h32[4 * j : 4 * j + 4, :] = rg[j].astype(F32)
    down = contract_last(h32[...].astype(BF16), wdg[...].reshape(256, 1024))
    for j in range(8):
        mh[j] = down[4 * j : 4 * j + 4].astype(BF16)
    rh[t] = mh[t]
    send(14, lambda i: mh.at[lax.bitwise_xor(t, i)], rh.at[t], ts)
    arrive(14, rh)
    last = res[t]
    summed = rh[0].astype(F32)
    for j in range(1, 8):
        summed += rh[j].astype(F32)
    done = (last + summed).astype(BF16)
    mi[...] = done
    ri[y] = done
    send(15, lambda i: mi, ri.at[y], ys)
    arrive(15, ri)
    for j in range(8):
        m32[4 * j : 4 * j + 4, :] = ri[j].astype(F32)
    out_ref[...] = contract_last(m32[...].astype(BF16), place_b)

    for n, buf in (
        (0, ra), (1, a2), (2, w1g), (3, w2g), (4, rb), (5, wmg), (6, rz1), (7, wug), (8, rz2), (9, wdg), (10, rc), (11, rd),
        (12, rf), (13, rg), (14, rh), (15, ri),
    ):
        left(n, buf)


def body(
    tokens, gain_mix, w_query, w_key, w_value, w_igate, w_fgate, bias_igate, bias_fgate, state_mem, state_max, keys_blk,
    values_blk, igate_blk, fgate_blk, lengths, gain_head, w_mixout, gain_mlp, w_up, w_down,
):
    args = (
        tokens, gain_mix.reshape(1, 32), w_query, w_key, w_value, w_igate.T, w_fgate.T, bias_igate.reshape(1, 1),
        bias_fgate.reshape(1, 1), state_mem, state_max.T, keys_blk, values_blk, igate_blk, fgate_blk, lengths.reshape(1, 4),
        gain_head.reshape(1, 256), w_mixout.T, gain_mlp.reshape(1, 32), w_up, w_down.T,
    )
    vm = pltpu.VMEM
    out = pl.pallas_call(
        kernel,
        out_shape=jax.ShapeDtypeStruct((32, 32), F32),
        in_specs=[pl.BlockSpec(memory_space=pl.ANY)] * 21,
        out_specs=pl.BlockSpec(memory_space=pltpu.VMEM),
        scratch_shapes=[
            vm((32, 32), BF16), vm((1, 32), F32), vm((1, 32), BF16), vm((1, 32), BF16), vm((1, 1), F32), vm((1, 1), F32),
            vm((4, 1, 256, 256), F32), vm((1, 4), F32), vm((4, 1, 128, 256), BF16), vm((4, 1, 128, 256), BF16),
            vm((4, 1, 128), F32), vm((4, 1, 128), F32), vm((1, 4), jnp.int32), vm((1, 256), F32), vm((1, 32), F32),
            vm((8, 32, 256), BF16), vm((8, 32, 512), BF16), vm((8, 32, 256), BF16), vm((8, 32, 1024), BF16),
            vm((8, 32, 1024), BF16),
            vm((8, 8, 256), BF16), vm((8, 8, 256), BF16), vm((8, 8, 256), BF16), vm((8, 256), BF16), vm((8, 8, 256), BF16),
            vm((32, 256), F32), vm((32, 256), F32), vm((8, 4, 384), BF16), vm((8, 4, 384), BF16), vm((8, 4, 512), BF16),
            vm((8, 4, 512), BF16), vm((4, 256, 256), BF16), vm((4, 256, 256), BF16), vm((3, 8, 128), F32), vm((16, 256), F32),
            vm((16, 128), F32), vm((4, 256), BF16), vm((8, 4, 256), BF16), vm((32, 256), F32), vm((32, 256), BF16),
            vm((8, 32, 256), BF16), vm((8, 4, 256), F32), vm((8, 4, 1152), BF16), vm((8, 4, 1152), BF16), vm((4, 1024), BF16),
            vm((8, 4, 1024), BF16), vm((32, 1024), F32), vm((8, 4, 256), BF16), vm((8, 4, 256), BF16), vm((4, 256), BF16),
            vm((8, 4, 256), BF16),
            pltpu.SemaphoreType.DMA((21,)), pltpu.SemaphoreType.DMA((16,)), pltpu.SemaphoreType.DMA((16,)),
        ],
        compiler_params=pltpu.CompilerParams(collective_id=0, has_side_effects=True),
    )(*args)
    return out.astype(BF16)


def solution(mesh):
    in_specs = (
        P("tp", "kv"),
        P("kv"),
        P("kv", "tp"),
        P("kv", "tp"),
        P("kv", "tp"),
        P("kv", "tp"),
        P("kv", "tp"),
        P("tp"),
        P("tp"),
        P("kv", "tp", None, None),
        P("kv", "tp"),
        P("kv", "tp", None, None),
        P("kv", "tp", None, None),
        P("kv", "tp", None),
        P("kv", "tp", None),
        P("kv"),
        P(),
        P("tp", "kv"),
        P("kv"),
        P("kv", "tp"),
        P("tp", "kv"),
    )
    return jax.shard_map(body, mesh=mesh, in_specs=in_specs, out_specs=P("tp", "kv"), check_vma=False)
```

```python
import jax
import jax.numpy as jnp
from jax import lax
from jax.experimental import pallas as pl
from jax.experimental.pallas import tpu as pltpu
from jax.sharding import PartitionSpec as P

MESH = pl.DeviceIdType.MESH
F32, BF16 = jnp.float32, jnp.bfloat16
D = 2048
EPS = 1e-06
SCALE = 256 ** (-0.5)


def at_lanes(rows, offset, width):
    lane = lax.broadcasted_iota(jnp.int32, (rows, width), 1)
    row = lax.broadcasted_iota(jnp.int32, (rows, width), 0)
    return jnp.where(lane == row + offset, 1.0, 0.0)


def contract_last(a, b):
    return lax.dot_general(a, b, (((1,), (1,)), ((), ())), preferred_element_type=F32)


def column(row_ref, rows):
    n = row_ref.shape[1]
    v = jnp.broadcast_to(row_ref[...].astype(F32), (rows, n))
    lane = lax.broadcasted_iota(jnp.int32, (rows, n), 1)
    row = lax.broadcasted_iota(jnp.int32, (rows, n), 0)
    return jnp.sum(jnp.where(lane == row, v, 0.0), axis=1, keepdims=True)


def kernel(
    tok_h, gmix_h, wq_h, wk_h, wv_h, wi_h, wf_h, bi_h, bf_h, st_h, smax_h, k_h, v_h, ig_h, fg_h, len_h, gh_h, wm_h, gm_h,
    wu_h, wd_h, out_ref,
    tok, gmix, wi, wf, bi, bfg, st, smax, kb, vb, igb, fgb, lens, gh, gm,
    w1g, w2g, wmg, wug, wdg,
    ma, ra, a2, xraw, mz1, rz1, mz2, rz2, slo, shi, rows8, q16, w16, mc, rc, m32, md, rd, mf, rf, mg, rg, h32,
    mh, rh, mp, rp,
    lsem, ssem, rsem,
):
    kv = lax.axis_index("kv")
    t = lax.axis_index("tp")
    z = lax.shift_right_logical(kv, 3)
    y = lax.bitwise_and(kv, 7)
    zs = lambda i: (lax.bitwise_xor(kv, 8 * i), t)
    ys = lambda i: (lax.bitwise_xor(kv, i), t)
    ts = lambda i: (kv, lax.bitwise_xor(t, i))

    far = z != t
    rows_to = lambda i: (8 * t + y, lax.bitwise_xor(t, i))
    rows_of = lambda i: (lax.bitwise_xor(kv, 8 * i), z)

    barrier = pltpu.get_barrier_semaphore()

    def greet(who):
        pl.semaphore_signal(barrier, inc=1, device_id=who, device_id_type=MESH)

    for who in (rows_to, rows_of, ys, zs, ts):
        for i in range(1, 8):
            greet(who(i))

    @pl.when(far)
    def _():
        greet(rows_to(0))
        greet(rows_of(0))

    loads = []

    def load(src, dst):
        c = pltpu.make_async_copy(src, dst, lsem.at[len(loads)])
        c.start()
        loads.append(c)
        return c

    l_tok = load(tok_h, tok)
    l_gmix = load(gmix_h, gmix)
    l_wi = load(wi_h, wi)
    l_wf = load(wf_h, wf)
    l_gm = load(gm_h, gm)
    l_w1 = load(wq_h, w1g.at[z])
    l_wk = load(wk_h, w2g.at[z, :, pl.ds(0, 256)])
    l_wv = load(wv_h, w2g.at[z, :, pl.ds(256, 256)])
    l_wm = load(wm_h, wmg.at[z])
    l_wu = load(wu_h, wug.at[z])
    l_wd = load(wd_h, wdg.at[z])
    cell = [
        load(a, b)
        for a, b in (
            (st_h, st), (smax_h, smax), (k_h, kb), (v_h, vb), (ig_h, igb), (fg_h, fgb), (len_h, lens), (gh_h, gh),
            (bi_h, bi), (bf_h, bfg),
        )
    ]

    pending, arrived = [], set()

    def send(n, src, buf, slot, who):
        dst = buf.at[slot]
        for i in range(1, 8):
            c = pltpu.make_async_remote_copy(
                src_ref=src(i), dst_ref=dst, send_sem=ssem.at[n], recv_sem=rsem.at[n], device_id=who(i), device_id_type=MESH
            )
            c.start()
        pending.append((n, buf))

    def arrive(n, buf):
        arrived.add(n)
        part = buf.at[pl.ds(0, 7)]
        pltpu.make_async_copy(part, part, rsem.at[n]).wait()

    def left(n, buf):
        part = buf.at[pl.ds(0, 7)]
        pltpu.make_async_copy(part, part, ssem.at[n]).wait()

    def start_one(n, src, dst, who):
        pltpu.make_async_remote_copy(
            src_ref=src, dst_ref=dst, send_sem=ssem.at[n], recv_sem=rsem.at[n], device_id=who, device_id_type=MESH
        ).start()

    def send_cross(n, src, buf, slot, who):
        for i in range(1, 8):
            start_one(n, src(i), buf.at[slot], who(i))

        @pl.when(far)
        def _():
            start_one(n, src(0), buf.at[slot], who(0))

        @pl.when(z == t)
        def _():
            buf[slot] = src(0)[...]

    zn = lambda k: lax.bitwise_and(z + k, 7)
    on_z = lambda k: (8 * zn(k) + y, t)

    def relay_copy(n, chunk, who, sem):
        pltpu.make_async_remote_copy(
            src_ref=chunk, dst_ref=chunk, send_sem=ssem.at[n], recv_sem=rsem.at[sem], device_id=who, device_id_type=MESH
        ).start()

    def spread(n, buf):
        for k in (2, -2, 1, -1):
            relay_copy(n, buf.at[z], on_z(k), n if abs(k) == 2 else 16 + n)
        pending.append((n, buf))
        arrived.add(n)

    def relay(n, buf):
        part = buf.at[pl.ds(0, 2)]
        pltpu.make_async_copy(part, part, rsem.at[n]).wait()
        half = buf.shape[2] // 2
        relay_copy(n, buf.at[zn(-2)], on_z(1), 32 + n)
        relay_copy(n, buf.at[zn(2)], on_z(-1), 32 + n)
        relay_copy(n, buf.at[zn(-2), :, pl.ds(0, half)], on_z(2), 32 + n)
        relay_copy(n, buf.at[zn(2), :, pl.ds(half, half)], on_z(-2), 32 + n)

    def collected(n, buf):
        part = buf.at[pl.ds(0, 2)]
        pltpu.make_async_copy(part, part, rsem.at[16 + n]).wait()
        part = buf.at[pl.ds(0, 3)]
        pltpu.make_async_copy(part, part, rsem.at[32 + n]).wait()

    def cross_done(sem, buf):
        @pl.when(far)
        def _():
            pltpu.make_async_copy(buf, buf, sem).wait()

        @pl.when(z == t)
        def _():
            part = buf.at[pl.ds(0, 7)]
            pltpu.make_async_copy(part, part, sem).wait()

    l_tok.wait()
    placed = jnp.dot(
        tok[...], at_lanes(32, 32 * lax.bitwise_and(z, 1), 128).astype(BF16), preferred_element_type=F32
    )
    ma[...] = (placed[0:16] + pltpu.roll(placed[16:32], 64, 1)).astype(BF16)
    pl.semaphore_wait(barrier, 37 - 2 * (z == t).astype(jnp.int32))
    send_cross(0, lambda i: ma, ra, z, rows_to)

    l_wi.wait()
    l_wf.wait()
    l_gm.wait()
    l_gmix.wait()

    def parts(g):
        first = g.astype(BF16).astype(F32)
        second = (g - first).astype(BF16).astype(F32)
        return first, second, g - first - second

    place = at_lanes(32, 32 * lax.bitwise_and(z, 3), 128).astype(BF16)
    row8 = lax.broadcasted_iota(jnp.int32, (8, 32), 0)
    eight = jnp.zeros((8, 32), F32)
    for r, v in enumerate((wi[...].astype(F32), wf[...].astype(F32), *parts(gm[...]), *parts(gmix[...]))):
        eight = jnp.where(row8 == r, jnp.broadcast_to(v, (8, 32)), eight)
    a2[z] = jnp.dot(eight.astype(BF16), place, preferred_element_type=F32).astype(BF16)
    send(1, lambda i: a2.at[z], a2, z, zs)
    l_w1.wait()
    spread(2, w1g)
    l_wk.wait()
    l_wv.wait()
    spread(3, w2g)

    for c in cell:
        c.wait()
    for s in range(4):
        hi = st[s, 0].astype(BF16)
        shi[s] = hi
        slo[s] = (st[s, 0] - hi.astype(F32)).astype(BF16)
    rows8[...] = jnp.zeros(rows8.shape, F32)
    for s in range(4):
        rows8[0, s : s + 1, :] = igb[s]
        rows8[1, s : s + 1, :] = fgb[s]
    lane = lax.broadcasted_iota(jnp.int32, (8, 128), 1)
    row = lax.broadcasted_iota(jnp.int32, (8, 128), 0)
    live = lane.astype(F32) < column(lens, 8)
    forget_live = jnp.where(live, rows8[1], 0.0)
    total = jnp.sum(forget_live, axis=1, keepdims=True)
    after = jnp.where(
        lax.broadcasted_iota(jnp.int32, (128, 128), 0) > lax.broadcasted_iota(jnp.int32, (128, 128), 1), 1.0, 0.0
    )
    past0 = rows8[0] + jnp.dot(forget_live, after, precision=lax.Precision.HIGHEST, preferred_element_type=F32)
    past0_top = jnp.max(jnp.where(live, past0, -1e30), axis=1, keepdims=True)
    carried0 = column(smax, 8) + total
    q16[...] = jnp.zeros(q16.shape, F32)
    w16[...] = jnp.zeros(w16.shape, F32)

    relay(2, w1g)
    relay(3, w2g)
    l_wm.wait()
    spread(5, wmg)
    cross_done(rsem.at[0], ra)
    low = lax.broadcasted_iota(jnp.int32, (16, 128), 1) < 64
    for h in range(2):
        one = ra[4 * h].astype(F32) + ra[4 * h + 1].astype(F32)
        two = ra[4 * h + 2].astype(F32) + ra[4 * h + 3].astype(F32)
        xraw[0:16, 128 * h : 128 * h + 128] = jnp.where(low, one, pltpu.roll(two, 64, 1))
        xraw[16:32, 128 * h : 128 * h + 128] = jnp.where(low, pltpu.roll(one, 64, 1), two)
    xr = xraw[...]
    square_in = jnp.sum(xr * xr, axis=1, keepdims=True)
    arrive(1, a2)
    halves = []
    for h in range(2):
        half = a2[4 * h].astype(F32)
        for j in range(1, 4):
            half += a2[4 * h + j].astype(F32)
        halves.append(half)
    small = jnp.concatenate(halves, axis=1)
    wgates = jnp.concatenate([small, jnp.zeros((120, 256), F32)], axis=0).astype(BF16)
    gain_mid = small[2:3] + small[3:4] + small[4:5]
    x = (xr * (small[5:6] + small[6:7] + small[7:8])).astype(BF16)
    lane32 = lax.broadcasted_iota(jnp.int32, (32, 128), 1)

    def with_square(block, sq, at):
        hi = sq.astype(BF16).astype(F32)
        return jnp.where(lane32 == at, hi, jnp.where(lane32 == at + 1, sq - hi, block))

    gates = with_square(contract_last(x, wgates), square_in, 2)
    collected(2, w1g)
    q_part = jnp.dot(x, w1g[...].reshape(256, 256), preferred_element_type=F32)
    for j in range(8):
        mz1[j, :, 0:256] = q_part[4 * j : 4 * j + 4].astype(BF16)
        mz1[j, :, 256:384] = gates[4 * j : 4 * j + 4].astype(BF16)
    rz1[y] = mz1[y]
    send(6, lambda i: mz1.at[lax.bitwise_xor(y, i)], rz1, y, ys)
    l_wu.wait()
    spread(7, wug)
    collected(3, w2g)
    kv_part = jnp.dot(x, w2g[...].reshape(256, 512), preferred_element_type=F32)
    for j in range(8):
        mz2[j] = kv_part[4 * j : 4 * j + 4].astype(BF16)
    rz2[y] = mz2[y]
    send(8, lambda i: mz2.at[lax.bitwise_xor(y, i)], rz2, y, ys)
    l_wd.wait()
    relay(5, wmg)
    spread(9, wdg)

    arrive(6, rz1)
    first = rz1[0].astype(F32)
    for j in range(1, 8):
        first += rz1[j].astype(F32)
    own = first[:, 256:384]
    factor = lax.rsqrt((own[:, 2:3] + own[:, 3:4]) / D + EPS)
    q16[0:4, :] = first[:, 0:256] * factor
    rows8[2, 0:4, :] = own * factor
    gate8 = rows8[2]
    input_gate = gate8[:, 0:1] + bi[...]
    pre = gate8[:, 1:2] + bfg[...]
    forget_gate = jnp.minimum(pre, 0.0) - jnp.log1p(jnp.exp(-jnp.abs(pre)))
    carried = carried0 + forget_gate
    topmost = jnp.maximum(jnp.maximum(carried, input_gate), past0_top + forget_gate)
    decay = jnp.where(live, jnp.exp(jnp.minimum(past0 + forget_gate - topmost, 0.0)), 0.0)
    qb = q16[...].astype(BF16)
    scores = jnp.zeros((8, 128), F32)
    state = jnp.zeros((8, 256), F32)
    row256 = lax.broadcasted_iota(jnp.int32, (8, 256), 0)
    for s in range(4):
        scores = jnp.where(row == s, contract_last(qb, kb[s, 0])[0:8], scores)
        part = contract_last(qb, shi[s])[0:8] + contract_last(qb, slo[s])[0:8]
        state = jnp.where(row256 == s, part, state)
    w16[0:8, :] = decay * (scores * SCALE)
    wb = w16[...].astype(BF16)
    block = jnp.zeros((8, 256), F32)
    for s in range(4):
        block = jnp.where(row256 == s, jnp.dot(wb, vb[s, 0], preferred_element_type=F32)[0:8], block)
    numerator = jnp.exp(carried - topmost) * state + block
    own_scale = jnp.exp(input_gate - topmost) * SCALE

    arrive(8, rz2)
    second = rz2[0].astype(F32)
    for j in range(1, 8):
        second += rz2[j].astype(F32)
    second = (second * factor).astype(BF16).astype(F32)
    own_score = jnp.sum(qb[0:4].astype(F32) * second[:, 0:256], axis=1, keepdims=True)
    num = numerator[0:4] + (own_scale[0:4] * own_score) * second[:, 256:512]
    mixed = num * lax.rsqrt(jnp.mean(num * num, axis=1, keepdims=True) + EPS) * gh[...]
    mc[...] = mixed.astype(BF16)
    rc[y] = mixed.astype(BF16)
    send(10, lambda i: mc, rc, y, ys)
    relay(7, wug)

    collected(5, wmg)
    arrive(10, rc)
    for j in range(8):
        m32[4 * j : 4 * j + 4, :] = rc[j].astype(F32)
    att = contract_last(m32[...].astype(BF16), wmg[...].reshape(256, 256)).astype(BF16)
    md[...] = att
    rd[t] = att
    send(11, lambda i: md, rd, t, ts)
    relay(9, wdg)
    arrive(11, rd)
    attended = rd[0].astype(F32)
    for j in range(1, 8):
        attended += rd[j].astype(F32)
    restored = (xraw[...] + attended).astype(BF16).astype(F32)
    sent = contract_last(restored.astype(BF16), at_lanes(32, 32 * t, 256).astype(BF16)).astype(BF16)
    mp[...] = sent

    @pl.when(far)
    def _():
        start_one(14, mp, rp, rows_to(lax.bitwise_xor(z, t)))

    @pl.when(z == t)
    def _():
        rp[...] = mp[...]

    square_mid = jnp.sum(restored * restored, axis=1, keepdims=True)
    sq_block = with_square(jnp.zeros((32, 128), F32), square_mid, 0)
    collected(7, wug)
    up = jnp.dot((restored * gain_mid).astype(BF16), wug[...].reshape(256, 1024), preferred_element_type=F32)
    for j in range(8):
        mf[j, :, 0:1024] = up[4 * j : 4 * j + 4].astype(BF16)
        mf[j, :, 1024:1152] = sq_block[4 * j : 4 * j + 4].astype(BF16)
    rf[y] = mf[y]
    send(12, lambda i: mf.at[lax.bitwise_xor(y, i)], rf, y, ys)
    arrive(12, rf)
    whole = rf[0].astype(F32)
    for j in range(1, 8):
        whole += rf[j].astype(F32)
    factor_mid = lax.rsqrt((whole[:, 1024:1025] + whole[:, 1025:1026]) / D + EPS)
    hid = jnp.square(jnp.maximum(whole[:, 0:1024] * factor_mid, 0.0)).astype(BF16)
    mg[...] = hid
    rg[y] = hid
    send(13, lambda i: mg, rg, y, ys)

    collected(9, wdg)
    arrive(13, rg)
    for j in range(8):
        h32[4 * j : 4 * j + 4, :] = rg[j].astype(F32)
    down = contract_last(h32[...].astype(BF16), wdg[...].reshape(256, 1024))
    for j in range(8):
        mh[j] = down[:, 32 * j : 32 * j + 32].astype(BF16)
    send_cross(15, lambda i: mh.at[lax.bitwise_xor(z, i)], rh, t, rows_of)

    @pl.when(far)
    def _():
        pltpu.make_async_copy(rp, rp, rsem.at[14]).wait()

    cross_done(rsem.at[15], rh)
    summed = rh[0].astype(F32)
    for j in range(1, 8):
        summed += rh[j].astype(F32)
    out_ref[...] = rp[...].astype(F32) + summed

    for n, buf in pending:
        left(n, buf)
    cross_done(ssem.at[0], ra)
    cross_done(ssem.at[15], rh)

    @pl.when(far)
    def _():
        pltpu.make_async_copy(mp, mp, ssem.at[14]).wait()


def body(
    tokens, gain_mix, w_query, w_key, w_value, w_igate, w_fgate, bias_igate, bias_fgate, state_mem, state_max, keys_blk,
    values_blk, igate_blk, fgate_blk, lengths, gain_head, w_mixout, gain_mlp, w_up, w_down,
):
    args = (
        tokens, gain_mix.reshape(1, 32), w_query, w_key, w_value, w_igate.T, w_fgate.T, bias_igate.reshape(1, 1),
        bias_fgate.reshape(1, 1), state_mem, state_max.T, keys_blk, values_blk, igate_blk, fgate_blk, lengths.reshape(1, 4),
        gain_head.reshape(1, 256), w_mixout.T, gain_mlp.reshape(1, 32), w_up, w_down.T,
    )
    vm = pltpu.VMEM
    out = pl.pallas_call(
        kernel,
        out_shape=jax.ShapeDtypeStruct((32, 32), F32),
        in_specs=[pl.BlockSpec(memory_space=pl.ANY)] * 21,
        out_specs=pl.BlockSpec(memory_space=pltpu.VMEM),
        scratch_shapes=[
            vm((32, 32), BF16), vm((1, 32), F32), vm((1, 32), BF16), vm((1, 32), BF16), vm((1, 1), F32), vm((1, 1), F32),
            vm((4, 1, 256, 256), F32), vm((1, 4), F32), vm((4, 1, 128, 256), BF16), vm((4, 1, 128, 256), BF16),
            vm((4, 1, 128), F32), vm((4, 1, 128), F32), vm((1, 4), jnp.int32), vm((1, 256), F32), vm((1, 32), F32),
            vm((8, 32, 256), BF16), vm((8, 32, 512), BF16), vm((8, 32, 256), BF16), vm((8, 32, 1024), BF16),
            vm((8, 32, 1024), BF16),
            vm((16, 128), BF16), vm((8, 16, 128), BF16), vm((8, 8, 128), BF16), vm((32, 256), F32), vm((8, 4, 384), BF16), vm((8, 4, 384), BF16), vm((8, 4, 512), BF16),
            vm((8, 4, 512), BF16), vm((4, 256, 256), BF16), vm((4, 256, 256), BF16), vm((3, 8, 128), F32), vm((16, 256), F32),
            vm((16, 128), F32), vm((4, 256), BF16), vm((8, 4, 256), BF16), vm((32, 256), F32), vm((32, 256), BF16),
            vm((8, 32, 256), BF16), vm((8, 4, 1152), BF16), vm((8, 4, 1152), BF16), vm((4, 1024), BF16),
            vm((8, 4, 1024), BF16), vm((32, 1024), F32), vm((8, 32, 32), BF16), vm((8, 32, 32), BF16), vm((32, 32), BF16),
            vm((32, 32), BF16),
            pltpu.SemaphoreType.DMA((21,)), pltpu.SemaphoreType.DMA((16,)), pltpu.SemaphoreType.DMA((48,)),
        ],
        compiler_params=pltpu.CompilerParams(collective_id=0, has_side_effects=True),
    )(*args)
    return out.astype(BF16)


def solution(mesh):
    in_specs = (
        P("tp", "kv"),
        P("kv"),
        P("kv", "tp"),
        P("kv", "tp"),
        P("kv", "tp"),
        P("kv", "tp"),
        P("kv", "tp"),
        P("tp"),
        P("tp"),
        P("kv", "tp", None, None),
        P("kv", "tp"),
        P("kv", "tp", None, None),
        P("kv", "tp", None, None),
        P("kv", "tp", None),
        P("kv", "tp", None),
        P("kv"),
        P(),
        P("tp", "kv"),
        P("kv"),
        P("kv", "tp"),
        P("tp", "kv"),
    )
    return jax.shard_map(body, mesh=mesh, in_specs=in_specs, out_specs=P("tp", "kv"), check_vma=False)
```

```python
import jax
import jax.numpy as jnp
from jax import lax
from jax.experimental import pallas as pl
from jax.experimental.pallas import tpu as pltpu
from jax.sharding import PartitionSpec as P

MESH = pl.DeviceIdType.MESH
F32, BF16 = jnp.float32, jnp.bfloat16
D = 2048
EPS = 1e-06
SCALE = 256 ** (-0.5)
T_FAR_FIRST = (4, 5, 6, 7, 2, 3, 1)
RING_FAR_FIRST = (4, 5, 3, 7, 6, 2, 1)


def at_lanes(rows, offset, width):
    lane = lax.broadcasted_iota(jnp.int32, (rows, width), 1)
    row = lax.broadcasted_iota(jnp.int32, (rows, width), 0)
    return jnp.where(lane == row + offset, 1.0, 0.0)


def contract_last(a, b):
    return lax.dot_general(a, b, (((1,), (1,)), ((), ())), preferred_element_type=F32)


def column(row_ref, rows):
    n = row_ref.shape[1]
    v = jnp.broadcast_to(row_ref[...].astype(F32), (rows, n))
    lane = lax.broadcasted_iota(jnp.int32, (rows, n), 1)
    row = lax.broadcasted_iota(jnp.int32, (rows, n), 0)
    return jnp.sum(jnp.where(lane == row, v, 0.0), axis=1, keepdims=True)


def kernel(
    tok_h, gmix_h, wq_h, wk_h, wv_h, wi_h, wf_h, bi_h, bf_h, st_h, smax_h, k_h, v_h, ig_h, fg_h, len_h, gh_h, wm_h, gm_h,
    wu_h, wd_h, out_ref,
    tok, gmix, wi, wf, bi, bfg, st, smax, kb, vb, igb, fgb, lens, gh, gm,
    w1g, w2g, wmg, wug, wdo, wdg,
    ma, ra, a2, xraw, mz1, rz1, mz2, rz2, slo, shi, rows8, q16, w16, mc, rc, m32, md, rd, mf, rf,
    mh, rh, mp, rp,
    lsem, ssem, rsem,
):
    kv = lax.axis_index("kv")
    t = lax.axis_index("tp")
    z = lax.shift_right_logical(kv, 3)
    y = lax.bitwise_and(kv, 7)
    zs = lambda i: (lax.bitwise_xor(kv, 8 * i), t)
    ys = lambda i: (lax.bitwise_xor(kv, i), t)
    ts = lambda i: (kv, lax.bitwise_xor(t, i))

    far = z != t
    rows_to = lambda i: (8 * t + y, lax.bitwise_xor(t, i))
    rows_of = lambda i: (lax.bitwise_xor(kv, 8 * i), z)

    barrier = pltpu.get_barrier_semaphore()

    def greet(who):
        pl.semaphore_signal(barrier, inc=1, device_id=who, device_id_type=MESH)

    @pl.when(far)
    def _():
        greet(rows_to(0))
        greet(rows_of(0))

    for i in T_FAR_FIRST:
        greet(rows_to(i))
    for who in (rows_of, zs, ys):
        for i in RING_FAR_FIRST:
            greet(who(i))
    for i in T_FAR_FIRST:
        greet(ts(i))

    loads = []

    def load(src, dst):
        c = pltpu.make_async_copy(src, dst, lsem.at[len(loads)])
        c.start()
        loads.append(c)
        return c

    l_tok = load(tok_h, tok)
    l_gmix = load(gmix_h, gmix)
    l_wi = load(wi_h, wi)
    l_wf = load(wf_h, wf)
    l_gm = load(gm_h, gm)
    l_w1 = load(wq_h, w1g.at[z])
    l_wk = load(wk_h, w2g.at[z, :, pl.ds(0, 256)])
    l_wv = load(wv_h, w2g.at[z, :, pl.ds(256, 256)])
    l_wm = load(wm_h, wmg.at[z])
    l_wu = load(wu_h, wug.at[z])
    own_units = pl.ds(pl.multiple_of(128 * y, 128), 128)
    l_wd = load(wd_h, wdo)
    l_wdy = load(wd_h.at[:, own_units], wdg.at[z, y])
    cell = [
        load(a, b)
        for a, b in (
            (st_h, st), (smax_h, smax), (k_h, kb), (v_h, vb), (ig_h, igb), (fg_h, fgb), (len_h, lens), (gh_h, gh),
            (bi_h, bi), (bf_h, bfg),
        )
    ]

    pending, arrived = [], set()

    def send(n, src, buf, slot, who):
        dst = buf.at[slot]
        for i in T_FAR_FIRST if who is ts else RING_FAR_FIRST:
            c = pltpu.make_async_remote_copy(
                src_ref=src(i), dst_ref=dst, send_sem=ssem.at[n], recv_sem=rsem.at[n], device_id=who(i), device_id_type=MESH
            )
            c.start()
        pending.append((n, buf))

    def arrive(n, buf):
        arrived.add(n)
        part = buf.at[pl.ds(0, 7)]
        pltpu.make_async_copy(part, part, rsem.at[n]).wait()

    def left(n, buf):
        part = buf.at[pl.ds(0, 7)]
        pltpu.make_async_copy(part, part, ssem.at[n]).wait()

    def start_one(n, src, dst, who):
        pltpu.make_async_remote_copy(
            src_ref=src, dst_ref=dst, send_sem=ssem.at[n], recv_sem=rsem.at[n], device_id=who, device_id_type=MESH
        ).start()

    def send_cross(n, src, buf, slot, who):
        for i in T_FAR_FIRST if who is rows_to else RING_FAR_FIRST:
            start_one(n, src(i), buf.at[slot], who(i))

        @pl.when(far)
        def _():
            start_one(n, src(0), buf.at[slot], who(0))

        @pl.when(z == t)
        def _():
            buf[slot] = src(0)[...]

    zn = lambda k: lax.bitwise_and(z + k, 7)
    on_z = lambda k: (8 * zn(k) + y, t)

    def relay_copy(n, chunk, who, sem):
        pltpu.make_async_remote_copy(
            src_ref=chunk, dst_ref=chunk, send_sem=ssem.at[n], recv_sem=rsem.at[sem], device_id=who, device_id_type=MESH
        ).start()

    def spread(n, buf, ks=(2, -2, 1, -1)):
        for k in ks:
            relay_copy(n, buf.at[z], on_z(k), n if abs(k) == 2 else 24 + n)
        if n not in arrived:
            pending.append((n, buf))
        arrived.add(n)

    def relay(n, buf):
        part = buf.at[pl.ds(0, 2)]
        pltpu.make_async_copy(part, part, rsem.at[n]).wait()
        half = buf.shape[2] // 2
        relay_copy(n, buf.at[zn(-2)], on_z(1), 48 + n)
        relay_copy(n, buf.at[zn(2)], on_z(-1), 48 + n)
        relay_copy(n, buf.at[zn(-2), :, pl.ds(0, half)], on_z(2), 48 + n)
        relay_copy(n, buf.at[zn(2), :, pl.ds(half, half)], on_z(-2), 48 + n)

    def collected(n, buf):
        part = buf.at[pl.ds(0, 2)]
        pltpu.make_async_copy(part, part, rsem.at[24 + n]).wait()
        part = buf.at[pl.ds(0, 3)]
        pltpu.make_async_copy(part, part, rsem.at[48 + n]).wait()

    def cross_done(sem, buf):
        @pl.when(far)
        def _():
            pltpu.make_async_copy(buf, buf, sem).wait()

        @pl.when(z == t)
        def _():
            part = buf.at[pl.ds(0, buf.shape[0] - 1)]
            pltpu.make_async_copy(part, part, sem).wait()

    l_tok.wait()
    placed = jnp.dot(
        tok[...], at_lanes(32, 32 * lax.bitwise_and(z, 1), 128).astype(BF16), preferred_element_type=F32
    )
    ma[...] = (placed[0:16] + pltpu.roll(placed[16:32], 64, 1)).astype(BF16)
    pl.semaphore_wait(barrier, 37 - 2 * (z == t).astype(jnp.int32))
    send_cross(0, lambda i: ma, ra, z, rows_to)

    l_wi.wait()
    l_wf.wait()
    l_gm.wait()
    l_gmix.wait()

    def parts(g):
        first = g.astype(BF16).astype(F32)
        second = (g - first).astype(BF16).astype(F32)
        return first, second, g - first - second

    place = at_lanes(32, 32 * lax.bitwise_and(z, 3), 128).astype(BF16)
    row8 = lax.broadcasted_iota(jnp.int32, (8, 32), 0)
    eight = jnp.zeros((8, 32), F32)
    for r, v in enumerate((wi[...].astype(F32), wf[...].astype(F32), *parts(gm[...]), *parts(gmix[...]))):
        eight = jnp.where(row8 == r, jnp.broadcast_to(v, (8, 32)), eight)
    a2[z] = jnp.dot(eight.astype(BF16), place, preferred_element_type=F32).astype(BF16)
    send(1, lambda i: a2.at[z], a2, z, zs)
    l_w1.wait()
    spread(2, w1g, (2, -2))
    l_wk.wait()
    l_wv.wait()
    spread(3, w2g, (2, -2))
    spread(2, w1g, (1, -1))
    spread(3, w2g, (1, -1))
    l_wd.wait()

    def units(i):
        return wdo.at[:, pl.ds(pl.multiple_of(128 * lax.bitwise_xor(y, i), 128), 128)]

    send(16, units, wdg.at[z], y, ys)

    for c in cell:
        c.wait()
    for s in range(4):
        hi = st[s, 0].astype(BF16)
        shi[s] = hi
        slo[s] = (st[s, 0] - hi.astype(F32)).astype(BF16)
    rows8[...] = jnp.zeros(rows8.shape, F32)
    for s in range(4):
        rows8[0, s : s + 1, :] = igb[s]
        rows8[1, s : s + 1, :] = fgb[s]
    lane = lax.broadcasted_iota(jnp.int32, (8, 128), 1)
    row = lax.broadcasted_iota(jnp.int32, (8, 128), 0)
    live = lane.astype(F32) < column(lens, 8)
    forget_live = jnp.where(live, rows8[1], 0.0)
    total = jnp.sum(forget_live, axis=1, keepdims=True)
    after = jnp.where(
        lax.broadcasted_iota(jnp.int32, (128, 128), 0) > lax.broadcasted_iota(jnp.int32, (128, 128), 1), 1.0, 0.0
    )
    past0 = rows8[0] + jnp.dot(forget_live, after, precision=lax.Precision.HIGHEST, preferred_element_type=F32)
    past0_top = jnp.max(jnp.where(live, past0, -1e30), axis=1, keepdims=True)
    carried0 = column(smax, 8) + total
    q16[...] = jnp.zeros(q16.shape, F32)
    w16[...] = jnp.zeros(w16.shape, F32)

    relay(2, w1g)
    relay(3, w2g)
    l_wm.wait()
    spread(5, wmg)
    cross_done(rsem.at[0], ra)
    low = lax.broadcasted_iota(jnp.int32, (16, 128), 1) < 64
    for h in range(2):
        one = ra[4 * h].astype(F32) + ra[4 * h + 1].astype(F32)
        two = ra[4 * h + 2].astype(F32) + ra[4 * h + 3].astype(F32)
        xraw[0:16, 128 * h : 128 * h + 128] = jnp.where(low, one, pltpu.roll(two, 64, 1))
        xraw[16:32, 128 * h : 128 * h + 128] = jnp.where(low, pltpu.roll(one, 64, 1), two)
    xr = xraw[...]
    square_in = jnp.sum(xr * xr, axis=1, keepdims=True)
    arrive(1, a2)
    halves = []
    for h in range(2):
        half = a2[4 * h].astype(F32)
        for j in range(1, 4):
            half += a2[4 * h + j].astype(F32)
        halves.append(half)
    small = jnp.concatenate(halves, axis=1)
    wgates = jnp.concatenate([small, jnp.zeros((120, 256), F32)], axis=0).astype(BF16)
    gain_mid = small[2:3] + small[3:4] + small[4:5]
    x = (xr * (small[5:6] + small[6:7] + small[7:8])).astype(BF16)
    lane32 = lax.broadcasted_iota(jnp.int32, (32, 128), 1)

    def with_square(block, sq, at):
        hi = sq.astype(BF16).astype(F32)
        return jnp.where(lane32 == at, hi, jnp.where(lane32 == at + 1, sq - hi, block))

    gates = with_square(contract_last(x, wgates), square_in, 2)
    collected(2, w1g)
    q_part = jnp.dot(x, w1g[...].reshape(256, 256), preferred_element_type=F32)
    for j in range(8):
        mz1[j, :, 0:256] = q_part[4 * j : 4 * j + 4].astype(BF16)
        mz1[j, :, 256:384] = gates[4 * j : 4 * j + 4].astype(BF16)
    rz1[y] = mz1[y]
    send(6, lambda i: mz1.at[lax.bitwise_xor(y, i)], rz1, y, ys)
    l_wu.wait()
    spread(7, wug)
    collected(3, w2g)
    kv_part = jnp.dot(x, w2g[...].reshape(256, 512), preferred_element_type=F32)
    for j in range(8):
        mz2[j] = kv_part[4 * j : 4 * j + 4].astype(BF16)
    rz2[y] = mz2[y]
    send(8, lambda i: mz2.at[lax.bitwise_xor(y, i)], rz2, y, ys)
    relay(5, wmg)
    l_wdy.wait()
    arrive(16, wdg.at[z])
    spread(9, wdg)

    arrive(6, rz1)
    first = rz1[0].astype(F32)
    for j in range(1, 8):
        first += rz1[j].astype(F32)
    own = first[:, 256:384]
    factor = lax.rsqrt((own[:, 2:3] + own[:, 3:4]) / D + EPS)
    q16[0:4, :] = first[:, 0:256] * factor
    rows8[2, 0:4, :] = own * factor
    gate8 = rows8[2]
    input_gate = gate8[:, 0:1] + bi[...]
    pre = gate8[:, 1:2] + bfg[...]
    forget_gate = jnp.minimum(pre, 0.0) - jnp.log1p(jnp.exp(-jnp.abs(pre)))
    carried = carried0 + forget_gate
    topmost = jnp.maximum(jnp.maximum(carried, input_gate), past0_top + forget_gate)
    decay = jnp.where(live, jnp.exp(jnp.minimum(past0 + forget_gate - topmost, 0.0)), 0.0)
    qb = q16[...].astype(BF16)
    scores = jnp.zeros((8, 128), F32)
    state = jnp.zeros((8, 256), F32)
    row256 = lax.broadcasted_iota(jnp.int32, (8, 256), 0)
    for s in range(4):
        scores = jnp.where(row == s, contract_last(qb, kb[s, 0])[0:8], scores)
        part = contract_last(qb, shi[s])[0:8] + contract_last(qb, slo[s])[0:8]
        state = jnp.where(row256 == s, part, state)
    w16[0:8, :] = decay * (scores * SCALE)
    wb = w16[...].astype(BF16)
    block = jnp.zeros((8, 256), F32)
    for s in range(4):
        block = jnp.where(row256 == s, jnp.dot(wb, vb[s, 0], preferred_element_type=F32)[0:8], block)
    numerator = jnp.exp(carried - topmost) * state + block
    own_scale = jnp.exp(input_gate - topmost) * SCALE

    arrive(8, rz2)
    second = rz2[0].astype(F32)
    for j in range(1, 8):
        second += rz2[j].astype(F32)
    second = (second * factor).astype(BF16).astype(F32)
    own_score = jnp.sum(qb[0:4].astype(F32) * second[:, 0:256], axis=1, keepdims=True)
    num = numerator[0:4] + (own_scale[0:4] * own_score) * second[:, 256:512]
    mixed = num * lax.rsqrt(jnp.mean(num * num, axis=1, keepdims=True) + EPS) * gh[...]
    mc[...] = mixed.astype(BF16)
    rc[y] = mixed.astype(BF16)
    send(10, lambda i: mc, rc, y, ys)
    relay(7, wug)

    collected(5, wmg)
    arrive(10, rc)
    for j in range(8):
        m32[4 * j : 4 * j + 4, :] = rc[j].astype(F32)
    att = contract_last(m32[...].astype(BF16), wmg[...].reshape(256, 256)).astype(BF16)
    md[...] = att
    rd[t] = att
    send(11, lambda i: md, rd, t, ts)
    relay(9, wdg)
    arrive(11, rd)
    attended = rd[0].astype(F32)
    for j in range(1, 8):
        attended += rd[j].astype(F32)
    restored = (xraw[...] + attended).astype(BF16).astype(F32)
    sent = contract_last(restored.astype(BF16), at_lanes(32, 32 * t, 256).astype(BF16)).astype(BF16)
    mp[...] = sent

    @pl.when(far)
    def _():
        start_one(14, mp, rp, rows_to(lax.bitwise_xor(z, t)))

    @pl.when(z == t)
    def _():
        rp[...] = mp[...]

    square_mid = jnp.sum(restored * restored, axis=1, keepdims=True)
    tile = lax.broadcasted_iota(jnp.int32, (8, 128), 1)
    high = square_mid.astype(BF16).astype(F32)
    sq_rows = jnp.zeros((8, 128), F32)
    for g in range(4):
        sq_rows = jnp.where(tile == g, high[8 * g : 8 * g + 8], sq_rows)
        sq_rows = jnp.where(tile == 4 + g, (square_mid - high)[8 * g : 8 * g + 8], sq_rows)
    sq_rows = jnp.concatenate([sq_rows, jnp.zeros((8, 128), F32)], axis=0).astype(BF16)
    collected(7, wug)
    up = jnp.dot((restored * gain_mid).astype(BF16), wug[...].reshape(256, 1024), preferred_element_type=F32)
    for j in range(8):
        mf[j, 0:32, :] = up[:, 128 * j : 128 * j + 128].astype(BF16)
        mf[j, 32:48, :] = sq_rows
    rf[y] = mf[y]
    send(12, lambda i: mf.at[lax.bitwise_xor(y, i)], rf, y, ys)
    arrive(12, rf)
    whole = rf[0].astype(F32)
    for j in range(1, 8):
        whole += rf[j].astype(F32)
    squares = jnp.concatenate(
        [whole[32:40, g : g + 1] + whole[32:40, 4 + g : 5 + g] for g in range(4)], axis=0
    )
    factor_mid = lax.rsqrt(squares / D + EPS)
    hid = jnp.square(jnp.maximum(whole[0:32] * factor_mid, 0.0)).astype(BF16)

    group = lax.shift_right_logical(tile, 5)
    collected(9, wdg)
    for jj in (*RING_FAR_FIRST, 0):
        zz = lax.bitwise_xor(z, jj)
        down = contract_last(hid, wdg[zz].reshape(256, 128))
        for h in range(2):
            part = down[:, 128 * h : 128 * h + 128]
            turned = [part] + [pltpu.roll(part, 32 * k, 1) for k in range(1, 4)]
            for d in range(4):
                packed = jnp.zeros((8, 128), F32)
                for g in range(4):
                    packed = jnp.where(group == g, turned[(g - d) % 4][8 * g : 8 * g + 8], packed)
                mh[8 * jj + 4 * h + d] = packed.astype(BF16)
        for i in (*RING_FAR_FIRST, 0) if jj else RING_FAR_FIRST:
            yy = lax.bitwise_xor(y, i)
            start_one(15, mh.at[8 * jj + yy], rh.at[8 * t + y], (8 * zz + yy, z))

    @pl.when(far)
    def _():
        start_one(15, mh.at[y], rh.at[8 * t + y], (kv, z))

    @pl.when(z == t)
    def _():
        rh[8 * t + y] = mh[y]

    @pl.when(far)
    def _():
        pltpu.make_async_copy(rp, rp, rsem.at[14]).wait()

    cross_done(rsem.at[15], rh)
    summed = rh[0].astype(F32)
    for j in range(1, 64):
        summed += rh[j].astype(F32)
    for g in range(4):
        rows = slice(8 * g, 8 * g + 8)
        out_ref[rows, :] = rp[rows, :].astype(F32) + summed[:, 32 * g : 32 * g + 32]

    for n, buf in pending:
        left(n, buf)
    cross_done(ssem.at[0], ra)
    cross_done(ssem.at[15], rh)

    @pl.when(far)
    def _():
        pltpu.make_async_copy(mp, mp, ssem.at[14]).wait()


def body(
    tokens, gain_mix, w_query, w_key, w_value, w_igate, w_fgate, bias_igate, bias_fgate, state_mem, state_max, keys_blk,
    values_blk, igate_blk, fgate_blk, lengths, gain_head, w_mixout, gain_mlp, w_up, w_down,
):
    args = (
        tokens, gain_mix.reshape(1, 32), w_query, w_key, w_value, w_igate.T, w_fgate.T, bias_igate.reshape(1, 1),
        bias_fgate.reshape(1, 1), state_mem, state_max.T, keys_blk, values_blk, igate_blk, fgate_blk, lengths.reshape(1, 4),
        gain_head.reshape(1, 256), w_mixout.T, gain_mlp.reshape(1, 32), w_up, w_down.T,
    )
    vm = pltpu.VMEM
    out = pl.pallas_call(
        kernel,
        out_shape=pltpu.VMEM((32, 32), F32),
        in_specs=[pl.BlockSpec(memory_space=pl.ANY)] * 21,
        out_specs=pl.BlockSpec(memory_space=pltpu.VMEM),
        scratch_shapes=[
            vm((32, 32), BF16), vm((1, 32), F32), vm((1, 32), BF16), vm((1, 32), BF16), vm((1, 1), F32), vm((1, 1), F32),
            vm((4, 1, 256, 256), F32), vm((1, 4), F32), vm((4, 1, 128, 256), BF16), vm((4, 1, 128, 256), BF16),
            vm((4, 1, 128), F32), vm((4, 1, 128), F32), vm((1, 4), jnp.int32), vm((1, 256), F32), vm((1, 32), F32),
            vm((8, 32, 256), BF16), vm((8, 32, 512), BF16), vm((8, 32, 256), BF16), vm((8, 32, 1024), BF16),
            vm((32, 1024), BF16), vm((8, 8, 32, 128), BF16),
            vm((16, 128), BF16), vm((8, 16, 128), BF16), vm((8, 8, 128), BF16), vm((32, 256), F32), vm((8, 4, 384), BF16), vm((8, 4, 384), BF16), vm((8, 4, 512), BF16),
            vm((8, 4, 512), BF16), vm((4, 256, 256), BF16), vm((4, 256, 256), BF16), vm((3, 8, 128), F32), vm((16, 256), F32),
            vm((16, 128), F32), vm((4, 256), BF16), vm((8, 4, 256), BF16), vm((32, 256), F32), vm((32, 256), BF16),
            vm((8, 32, 256), BF16), vm((8, 48, 128), BF16), vm((8, 48, 128), BF16),
            vm((64, 8, 128), BF16), vm((64, 8, 128), BF16), vm((32, 32), BF16),
            vm((32, 32), BF16),
            pltpu.SemaphoreType.DMA((22,)), pltpu.SemaphoreType.DMA((24,)), pltpu.SemaphoreType.DMA((72,)),
        ],
        compiler_params=pltpu.CompilerParams(collective_id=0, has_side_effects=True),
    )(*args)
    return out.astype(BF16)


def solution(mesh):
    in_specs = (
        P("tp", "kv"),
        P("kv"),
        P("kv", "tp"),
        P("kv", "tp"),
        P("kv", "tp"),
        P("kv", "tp"),
        P("kv", "tp"),
        P("tp"),
        P("tp"),
        P("kv", "tp", None, None),
        P("kv", "tp"),
        P("kv", "tp", None, None),
        P("kv", "tp", None, None),
        P("kv", "tp", None),
        P("kv", "tp", None),
        P("kv"),
        P(),
        P("tp", "kv"),
        P("kv"),
        P("kv", "tp"),
        P("tp", "kv"),
    )
    return jax.shard_map(body, mesh=mesh, in_specs=in_specs, out_specs=P("tp", "kv"), check_vma=False)
```

```python
import jax
import jax.numpy as jnp
from jax import lax
from jax.experimental import pallas as pl
from jax.experimental.pallas import tpu as pltpu
from jax.sharding import PartitionSpec as P

MESH = pl.DeviceIdType.MESH
F32, BF16 = jnp.float32, jnp.bfloat16
D = 2048
EPS = 1e-06
SCALE = 256 ** (-0.5)
T_FAR_FIRST = (4, 5, 6, 7, 2, 3, 1)
RING_FAR_FIRST = (4, 5, 3, 7, 6, 2, 1)


def at_lanes(rows, offset, width):
    lane = lax.broadcasted_iota(jnp.int32, (rows, width), 1)
    row = lax.broadcasted_iota(jnp.int32, (rows, width), 0)
    return jnp.where(lane == row + offset, 1.0, 0.0)


def contract_last(a, b):
    return lax.dot_general(a, b, (((1,), (1,)), ((), ())), preferred_element_type=F32)


def column(row_ref, rows):
    n = row_ref.shape[1]
    v = jnp.broadcast_to(row_ref[...].astype(F32), (rows, n))
    lane = lax.broadcasted_iota(jnp.int32, (rows, n), 1)
    row = lax.broadcasted_iota(jnp.int32, (rows, n), 0)
    return jnp.sum(jnp.where(lane == row, v, 0.0), axis=1, keepdims=True)


def kernel(
    tok_h, gmix_h, wq_h, wk_h, wv_h, wi_h, wf_h, bi_h, bf_h, st_h, smax_h, k_h, v_h, ig_h, fg_h, len_h, gh_h, wm_h, gm_h,
    wu_h, wd_h, out_ref,
    tok, gmix, wi, wf, bi, bfg, st, smax, kb, vb, igb, fgb, lens, gh, gm,
    w1g, w2g, wmg, wug, wdo, wdg,
    ma, ra, a2, xraw, mz1, rz1, mz2, rz2, slo, shi, rows8, q16, w16, mc, rc, m32, md, rd, mf, rf,
    mh, rh, mp, rp,
    lsem, ssem, rsem,
):
    kv = lax.axis_index("kv")
    t = lax.axis_index("tp")
    z = lax.shift_right_logical(kv, 3)
    y = lax.bitwise_and(kv, 7)
    zs = lambda i: (lax.bitwise_xor(kv, 8 * i), t)
    ys = lambda i: (lax.bitwise_xor(kv, i), t)
    ts = lambda i: (kv, lax.bitwise_xor(t, i))

    far = z != t
    rows_to = lambda i: (8 * t + y, lax.bitwise_xor(t, i))
    rows_of = lambda i: (lax.bitwise_xor(kv, 8 * i), z)

    barrier = pltpu.get_barrier_semaphore()

    def greet(who):
        pl.semaphore_signal(barrier, inc=1, device_id=who, device_id_type=MESH)

    @pl.when(far)
    def _():
        greet(rows_to(0))
        greet(rows_of(0))

    for i in T_FAR_FIRST:
        greet(rows_to(i))
    for who in (rows_of, zs, ys):
        for i in RING_FAR_FIRST:
            greet(who(i))

    loads = []

    def load(src, dst):
        c = pltpu.make_async_copy(src, dst, lsem.at[len(loads)])
        c.start()
        loads.append(c)
        return c

    l_tok = load(tok_h, tok)
    l_gmix = load(gmix_h, gmix)
    l_wi = load(wi_h, wi)
    l_wf = load(wf_h, wf)
    l_gm = load(gm_h, gm)
    l_w1 = load(wq_h, w1g.at[z])
    l_wk = load(wk_h, w2g.at[z, :, pl.ds(0, 256)])
    l_wv = load(wv_h, w2g.at[z, :, pl.ds(256, 256)])
    l_wm = load(wm_h, wmg.at[z])
    l_wu = load(wu_h, wug.at[z])
    own_units = pl.ds(pl.multiple_of(128 * y, 128), 128)
    l_wd = load(wd_h, wdo)
    l_wdy = load(wd_h.at[:, own_units], wdg.at[z, y])
    cell = [
        load(a, b)
        for a, b in (
            (st_h, st), (smax_h, smax), (k_h, kb), (v_h, vb), (ig_h, igb), (fg_h, fgb), (len_h, lens), (gh_h, gh),
            (bi_h, bi), (bf_h, bfg),
        )
    ]

    pending, arrived = [], set()

    def send(n, src, buf, slot, who):
        dst = buf.at[slot]
        for i in T_FAR_FIRST if who is ts else RING_FAR_FIRST:
            c = pltpu.make_async_remote_copy(
                src_ref=src(i), dst_ref=dst, send_sem=ssem.at[n], recv_sem=rsem.at[n], device_id=who(i), device_id_type=MESH
            )
            c.start()
        pending.append((n, buf))

    def arrive(n, buf):
        arrived.add(n)
        part = buf.at[pl.ds(0, 7)]
        pltpu.make_async_copy(part, part, rsem.at[n]).wait()

    def left(n, buf):
        part = buf.at[pl.ds(0, 7)]
        pltpu.make_async_copy(part, part, ssem.at[n]).wait()

    def start_one(n, src, dst, who):
        pltpu.make_async_remote_copy(
            src_ref=src, dst_ref=dst, send_sem=ssem.at[n], recv_sem=rsem.at[n], device_id=who, device_id_type=MESH
        ).start()

    def send_cross(n, src, buf, slot, who):
        for i in T_FAR_FIRST if who is rows_to else RING_FAR_FIRST:
            start_one(n, src(i), buf.at[slot], who(i))

        @pl.when(far)
        def _():
            start_one(n, src(0), buf.at[slot], who(0))

        @pl.when(z == t)
        def _():
            buf[slot] = src(0)[...]

    zn = lambda k: lax.bitwise_and(z + k, 7)
    on_z = lambda k: (8 * zn(k) + y, t)

    def relay_copy(n, chunk, who, sem):
        pltpu.make_async_remote_copy(
            src_ref=chunk, dst_ref=chunk, send_sem=ssem.at[n], recv_sem=rsem.at[sem], device_id=who, device_id_type=MESH
        ).start()

    def spread(n, buf, ks=(2, -2, 1, -1)):
        for k in ks:
            relay_copy(n, buf.at[z], on_z(k), n if abs(k) == 2 else 24 + n)
        if n not in arrived:
            pending.append((n, buf))
        arrived.add(n)

    def relay(n, buf):
        part = buf.at[pl.ds(0, 2)]
        pltpu.make_async_copy(part, part, rsem.at[n]).wait()
        half = buf.shape[2] // 2
        relay_copy(n, buf.at[zn(-2), :, pl.ds(0, half)], on_z(2), 48 + n)
        relay_copy(n, buf.at[zn(2), :, pl.ds(half, half)], on_z(-2), 48 + n)
        relay_copy(n, buf.at[zn(-2)], on_z(1), 48 + n)
        relay_copy(n, buf.at[zn(2)], on_z(-1), 48 + n)

    def collected(n, buf):
        part = buf.at[pl.ds(0, 2)]
        pltpu.make_async_copy(part, part, rsem.at[24 + n]).wait()
        part = buf.at[pl.ds(0, 3)]
        pltpu.make_async_copy(part, part, rsem.at[48 + n]).wait()

    def cross_done(sem, buf):
        @pl.when(far)
        def _():
            pltpu.make_async_copy(buf, buf, sem).wait()

        @pl.when(z == t)
        def _():
            part = buf.at[pl.ds(0, buf.shape[0] - 1)]
            pltpu.make_async_copy(part, part, sem).wait()

    l_tok.wait()
    placed = jnp.dot(
        tok[...], at_lanes(32, 32 * lax.bitwise_and(z, 1), 128).astype(BF16), preferred_element_type=F32
    )
    ma[...] = (placed[0:16] + pltpu.roll(placed[16:32], 64, 1)).astype(BF16)
    pl.semaphore_wait(barrier, 30 - 2 * (z == t).astype(jnp.int32))
    send_cross(0, lambda i: ma, ra, z, rows_to)

    l_wi.wait()
    l_wf.wait()
    l_gm.wait()
    l_gmix.wait()

    def parts(g):
        first = g.astype(BF16).astype(F32)
        second = (g - first).astype(BF16).astype(F32)
        return first, second, g - first - second

    place = at_lanes(32, 32 * lax.bitwise_and(z, 3), 128).astype(BF16)
    row8 = lax.broadcasted_iota(jnp.int32, (8, 32), 0)
    eight = jnp.zeros((8, 32), F32)
    for r, v in enumerate((wi[...].astype(F32), wf[...].astype(F32), *parts(gm[...]), *parts(gmix[...]))):
        eight = jnp.where(row8 == r, jnp.broadcast_to(v, (8, 32)), eight)
    a2[z] = jnp.dot(eight.astype(BF16), place, preferred_element_type=F32).astype(BF16)
    l_w1.wait()
    spread(2, w1g, (2, -2))
    l_wk.wait()
    l_wv.wait()
    spread(3, w2g, (2, -2))
    spread(2, w1g, (1, -1))
    send(1, lambda i: a2.at[z], a2, z, zs)
    spread(3, w2g, (1, -1))
    l_wd.wait()

    def units(i):
        return wdo.at[:, pl.ds(pl.multiple_of(128 * lax.bitwise_xor(y, i), 128), 128)]

    send(16, units, wdg.at[z], y, ys)

    for c in cell:
        c.wait()
    rows8[...] = jnp.zeros(rows8.shape, F32)
    for s in range(4):
        rows8[0, s : s + 1, :] = igb[s]
        rows8[1, s : s + 1, :] = fgb[s]
    lane = lax.broadcasted_iota(jnp.int32, (8, 128), 1)
    row = lax.broadcasted_iota(jnp.int32, (8, 128), 0)
    live = lane.astype(F32) < column(lens, 8)
    forget_live = jnp.where(live, rows8[1], 0.0)
    total = jnp.sum(forget_live, axis=1, keepdims=True)
    after = jnp.where(
        lax.broadcasted_iota(jnp.int32, (128, 128), 0) > lax.broadcasted_iota(jnp.int32, (128, 128), 1), 1.0, 0.0
    )
    past0 = rows8[0] + jnp.dot(forget_live, after, precision=lax.Precision.HIGHEST, preferred_element_type=F32)
    past0_top = jnp.max(jnp.where(live, past0, -1e30), axis=1, keepdims=True)
    carried0 = column(smax, 8) + total
    q16[...] = jnp.zeros(q16.shape, F32)
    w16[...] = jnp.zeros(w16.shape, F32)

    relay(2, w1g)
    relay(3, w2g)
    l_wm.wait()
    spread(5, wmg)
    cross_done(rsem.at[0], ra)
    low = lax.broadcasted_iota(jnp.int32, (16, 128), 1) < 64
    for h in range(2):
        one = ra[4 * h].astype(F32) + ra[4 * h + 1].astype(F32)
        two = ra[4 * h + 2].astype(F32) + ra[4 * h + 3].astype(F32)
        xraw[0:16, 128 * h : 128 * h + 128] = jnp.where(low, one, pltpu.roll(two, 64, 1))
        xraw[16:32, 128 * h : 128 * h + 128] = jnp.where(low, pltpu.roll(one, 64, 1), two)
    xr = xraw[...]
    square_in = jnp.sum(xr * xr, axis=1, keepdims=True)
    arrive(1, a2)
    halves = []
    for h in range(2):
        half = a2[4 * h].astype(F32)
        for j in range(1, 4):
            half += a2[4 * h + j].astype(F32)
        halves.append(half)
    small = jnp.concatenate(halves, axis=1)
    wgates = jnp.concatenate([small, jnp.zeros((120, 256), F32)], axis=0).astype(BF16)
    gain_mid = small[2:3] + small[3:4] + small[4:5]
    x = (xr * (small[5:6] + small[6:7] + small[7:8])).astype(BF16)
    lane32 = lax.broadcasted_iota(jnp.int32, (32, 128), 1)

    def with_square(block, sq, at):
        hi = sq.astype(BF16).astype(F32)
        return jnp.where(lane32 == at, hi, jnp.where(lane32 == at + 1, sq - hi, block))

    gates = with_square(contract_last(x, wgates), square_in, 2)
    collected(2, w1g)
    q_part = jnp.dot(x, w1g[...].reshape(256, 256), preferred_element_type=F32)
    for j in range(8):
        mz1[j, :, 0:256] = q_part[4 * j : 4 * j + 4].astype(BF16)
        mz1[j, :, 256:384] = gates[4 * j : 4 * j + 4].astype(BF16)
    rz1[y] = mz1[y]
    send(6, lambda i: mz1.at[lax.bitwise_xor(y, i)], rz1, y, ys)
    l_wu.wait()
    spread(7, wug)
    collected(3, w2g)
    kv_part = jnp.dot(x, w2g[...].reshape(256, 512), preferred_element_type=F32)
    for j in range(8):
        mz2[j] = kv_part[4 * j : 4 * j + 4].astype(BF16)
    rz2[y] = mz2[y]
    send(8, lambda i: mz2.at[lax.bitwise_xor(y, i)], rz2, y, ys)
    relay(5, wmg)
    l_wdy.wait()
    arrive(16, wdg.at[z])
    spread(9, wdg)

    for s in range(4):
        hi = st[s, 0].astype(BF16)
        shi[s] = hi
        slo[s] = (st[s, 0] - hi.astype(F32)).astype(BF16)
    arrive(6, rz1)
    first = rz1[0].astype(F32)
    for j in range(1, 8):
        first += rz1[j].astype(F32)
    own = first[:, 256:384]
    factor = lax.rsqrt((own[:, 2:3] + own[:, 3:4]) / D + EPS)
    q16[0:4, :] = first[:, 0:256] * factor
    rows8[2, 0:4, :] = own * factor
    gate8 = rows8[2]
    input_gate = gate8[:, 0:1] + bi[...]
    pre = gate8[:, 1:2] + bfg[...]
    forget_gate = jnp.minimum(pre, 0.0) - jnp.log1p(jnp.exp(-jnp.abs(pre)))
    carried = carried0 + forget_gate
    topmost = jnp.maximum(jnp.maximum(carried, input_gate), past0_top + forget_gate)
    decay = jnp.where(live, jnp.exp(jnp.minimum(past0 + forget_gate - topmost, 0.0)), 0.0)
    qb = q16[...].astype(BF16)
    scores = jnp.zeros((8, 128), F32)
    state = jnp.zeros((8, 256), F32)
    row256 = lax.broadcasted_iota(jnp.int32, (8, 256), 0)
    for s in range(4):
        scores = jnp.where(row == s, contract_last(qb, kb[s, 0])[0:8], scores)
        part = contract_last(qb, shi[s])[0:8] + contract_last(qb, slo[s])[0:8]
        state = jnp.where(row256 == s, part, state)
    w16[0:8, :] = decay * (scores * SCALE)
    wb = w16[...].astype(BF16)
    block = jnp.zeros((8, 256), F32)
    for s in range(4):
        block = jnp.where(row256 == s, jnp.dot(wb, vb[s, 0], preferred_element_type=F32)[0:8], block)
    numerator = jnp.exp(carried - topmost) * state + block
    own_scale = jnp.exp(input_gate - topmost) * SCALE

    arrive(8, rz2)
    second = rz2[0].astype(F32)
    for j in range(1, 8):
        second += rz2[j].astype(F32)
    second = (second * factor).astype(BF16).astype(F32)
    own_score = jnp.sum(qb[0:4].astype(F32) * second[:, 0:256], axis=1, keepdims=True)
    num = numerator[0:4] + (own_scale[0:4] * own_score) * second[:, 256:512]
    mixed = num * lax.rsqrt(jnp.mean(num * num, axis=1, keepdims=True) + EPS) * gh[...]
    mc[...] = mixed.astype(BF16)
    rc[y] = mixed.astype(BF16)
    send(10, lambda i: mc, rc, y, ys)
    relay(7, wug)

    collected(5, wmg)
    arrive(10, rc)
    for j in range(8):
        m32[4 * j : 4 * j + 4, :] = rc[j].astype(F32)
    att = contract_last(m32[...].astype(BF16), wmg[...].reshape(256, 256)).astype(BF16)
    md[...] = att
    rd[t] = att
    send(11, lambda i: md, rd, t, ts)
    relay(9, wdg)
    arrive(11, rd)
    attended = rd[0].astype(F32)
    for j in range(1, 8):
        attended += rd[j].astype(F32)
    restored = (xraw[...] + attended).astype(BF16).astype(F32)
    sent = contract_last(restored.astype(BF16), at_lanes(32, 32 * t, 256).astype(BF16)).astype(BF16)
    mp[...] = sent

    @pl.when(far)
    def _():
        start_one(14, mp, rp, rows_to(lax.bitwise_xor(z, t)))

    @pl.when(z == t)
    def _():
        rp[...] = mp[...]

    square_mid = jnp.sum(restored * restored, axis=1, keepdims=True)
    tile = lax.broadcasted_iota(jnp.int32, (8, 128), 1)
    high = square_mid.astype(BF16).astype(F32)
    sq_rows = jnp.zeros((8, 128), F32)
    for g in range(4):
        sq_rows = jnp.where(tile == g, high[8 * g : 8 * g + 8], sq_rows)
        sq_rows = jnp.where(tile == 4 + g, (square_mid - high)[8 * g : 8 * g + 8], sq_rows)
    sq_rows = jnp.concatenate([sq_rows, jnp.zeros((8, 128), F32)], axis=0).astype(BF16)
    collected(7, wug)
    up = jnp.dot((restored * gain_mid).astype(BF16), wug[...].reshape(256, 1024), preferred_element_type=F32)
    for j in range(8):
        mf[j, 0:32, :] = up[:, 128 * j : 128 * j + 128].astype(BF16)
        mf[j, 32:48, :] = sq_rows
    rf[y] = mf[y]
    send(12, lambda i: mf.at[lax.bitwise_xor(y, i)], rf, y, ys)
    arrive(12, rf)
    whole = rf[0].astype(F32)
    for j in range(1, 8):
        whole += rf[j].astype(F32)
    squares = jnp.concatenate(
        [whole[32:40, g : g + 1] + whole[32:40, 4 + g : 5 + g] for g in range(4)], axis=0
    )
    factor_mid = lax.rsqrt(squares / D + EPS)
    hid = jnp.square(jnp.maximum(whole[0:32] * factor_mid, 0.0)).astype(BF16)

    group = lax.shift_right_logical(tile, 5)
    collected(9, wdg)
    for jj in (*RING_FAR_FIRST, 0):
        zz = lax.bitwise_xor(z, jj)
        down = contract_last(hid, wdg[zz].reshape(256, 128))
        for h in range(2):
            part = down[:, 128 * h : 128 * h + 128]
            turned = [part] + [pltpu.roll(part, 32 * k, 1) for k in range(1, 4)]
            for d in range(4):
                packed = jnp.zeros((8, 128), F32)
                for g in range(4):
                    packed = jnp.where(group == g, turned[(g - d) % 4][8 * g : 8 * g + 8], packed)
                mh[8 * jj + 4 * h + d] = packed.astype(BF16)
        for i in (*RING_FAR_FIRST, 0) if jj else RING_FAR_FIRST:
            yy = lax.bitwise_xor(y, i)
            start_one(15, mh.at[8 * jj + yy], rh.at[8 * t + y], (8 * zz + yy, z))

    @pl.when(far)
    def _():
        start_one(15, mh.at[y], rh.at[8 * t + y], (kv, z))

    @pl.when(z == t)
    def _():
        rh[8 * t + y] = mh[y]

    @pl.when(far)
    def _():
        pltpu.make_async_copy(rp, rp, rsem.at[14]).wait()

    cross_done(rsem.at[15], rh)
    summed = rh[0].astype(F32)
    for j in range(1, 64):
        summed += rh[j].astype(F32)
    for g in range(4):
        rows = slice(8 * g, 8 * g + 8)
        out_ref[rows, :] = rp[rows, :].astype(F32) + summed[:, 32 * g : 32 * g + 32]

    for n, buf in pending:
        left(n, buf)
    cross_done(ssem.at[0], ra)
    cross_done(ssem.at[15], rh)

    @pl.when(far)
    def _():
        pltpu.make_async_copy(mp, mp, ssem.at[14]).wait()


def body(
    tokens, gain_mix, w_query, w_key, w_value, w_igate, w_fgate, bias_igate, bias_fgate, state_mem, state_max, keys_blk,
    values_blk, igate_blk, fgate_blk, lengths, gain_head, w_mixout, gain_mlp, w_up, w_down,
):
    args = (
        tokens, gain_mix.reshape(1, 32), w_query, w_key, w_value, w_igate.T, w_fgate.T, bias_igate.reshape(1, 1),
        bias_fgate.reshape(1, 1), state_mem, state_max.T, keys_blk, values_blk, igate_blk, fgate_blk, lengths.reshape(1, 4),
        gain_head.reshape(1, 256), w_mixout.T, gain_mlp.reshape(1, 32), w_up, w_down.T,
    )
    vm = pltpu.VMEM
    out = pl.pallas_call(
        kernel,
        out_shape=pltpu.VMEM((32, 32), F32),
        in_specs=[pl.BlockSpec(memory_space=pl.ANY)] * 21,
        out_specs=pl.BlockSpec(memory_space=pltpu.VMEM),
        scratch_shapes=[
            vm((32, 32), BF16), vm((1, 32), F32), vm((1, 32), BF16), vm((1, 32), BF16), vm((1, 1), F32), vm((1, 1), F32),
            vm((4, 1, 256, 256), F32), vm((1, 4), F32), vm((4, 1, 128, 256), BF16), vm((4, 1, 128, 256), BF16),
            vm((4, 1, 128), F32), vm((4, 1, 128), F32), vm((1, 4), jnp.int32), vm((1, 256), F32), vm((1, 32), F32),
            vm((8, 32, 256), BF16), vm((8, 32, 512), BF16), vm((8, 32, 256), BF16), vm((8, 32, 1024), BF16),
            vm((32, 1024), BF16), vm((8, 8, 32, 128), BF16),
            vm((16, 128), BF16), vm((8, 16, 128), BF16), vm((8, 8, 128), BF16), vm((32, 256), F32), vm((8, 4, 384), BF16), vm((8, 4, 384), BF16), vm((8, 4, 512), BF16),
            vm((8, 4, 512), BF16), vm((4, 256, 256), BF16), vm((4, 256, 256), BF16), vm((3, 8, 128), F32), vm((16, 256), F32),
            vm((16, 128), F32), vm((4, 256), BF16), vm((8, 4, 256), BF16), vm((32, 256), F32), vm((32, 256), BF16),
            vm((8, 32, 256), BF16), vm((8, 48, 128), BF16), vm((8, 48, 128), BF16),
            vm((64, 8, 128), BF16), vm((64, 8, 128), BF16), vm((32, 32), BF16),
            vm((32, 32), BF16),
            pltpu.SemaphoreType.DMA((22,)), pltpu.SemaphoreType.DMA((24,)), pltpu.SemaphoreType.DMA((72,)),
        ],
        compiler_params=pltpu.CompilerParams(collective_id=0, has_side_effects=True),
    )(*args)
    return out.astype(BF16)


def solution(mesh):
    in_specs = (
        P("tp", "kv"),
        P("kv"),
        P("kv", "tp"),
        P("kv", "tp"),
        P("kv", "tp"),
        P("kv", "tp"),
        P("kv", "tp"),
        P("tp"),
        P("tp"),
        P("kv", "tp", None, None),
        P("kv", "tp"),
        P("kv", "tp", None, None),
        P("kv", "tp", None, None),
        P("kv", "tp", None),
        P("kv", "tp", None),
        P("kv"),
        P(),
        P("tp", "kv"),
        P("kv"),
        P("kv", "tp"),
        P("tp", "kv"),
    )
    return jax.shard_map(body, mesh=mesh, in_specs=in_specs, out_specs=P("tp", "kv"), check_vma=False)
```

```python
import jax
import jax.numpy as jnp
from jax import lax
from jax.experimental import pallas as pl
from jax.experimental.pallas import tpu as pltpu
from jax.sharding import PartitionSpec as P

MESH = pl.DeviceIdType.MESH
F32, BF16 = jnp.float32, jnp.bfloat16
D = 2048
EPS = 1e-06
SCALE = 256 ** (-0.5)
T_FAR_FIRST = (4, 5, 6, 7, 2, 3, 1)
RING_FAR_FIRST = (4, 5, 3, 7, 6, 2, 1)


def at_lanes(rows, offset, width):
    lane = lax.broadcasted_iota(jnp.int32, (rows, width), 1)
    row = lax.broadcasted_iota(jnp.int32, (rows, width), 0)
    return jnp.where(lane == row + offset, 1.0, 0.0)


def contract_last(a, b):
    return lax.dot_general(a, b, (((1,), (1,)), ((), ())), preferred_element_type=F32)


def column(row_ref, rows):
    n = row_ref.shape[1]
    v = jnp.broadcast_to(row_ref[...].astype(F32), (rows, n))
    lane = lax.broadcasted_iota(jnp.int32, (rows, n), 1)
    row = lax.broadcasted_iota(jnp.int32, (rows, n), 0)
    return jnp.sum(jnp.where(lane == row, v, 0.0), axis=1, keepdims=True)


def kernel(
    tok_h, gmix_h, wq_h, wk_h, wv_h, wi_h, wf_h, bi_h, bf_h, st_h, smax_h, k_h, v_h, ig_h, fg_h, len_h, gh_h, wm_h, gm_h,
    wu_h, wd_h, out_ref,
    tok, gmix, wi, wf, bi, bfg, st, smax, kb, vb, igb, fgb, lens, gh, gm,
    w1g, w2g, wmg, wug, wdo, wdg,
    ma, ra, a2, xraw, mz1, rz1, mz2, rz2, slo, shi, rows8, q16, w16, mc, rc, m32, md, rd, mf, rf,
    mh, rh, mp, rp,
    lsem, ssem, rsem,
):
    kv = lax.axis_index("kv")
    t = lax.axis_index("tp")
    z = lax.shift_right_logical(kv, 3)
    y = lax.bitwise_and(kv, 7)
    zs = lambda i: (lax.bitwise_xor(kv, 8 * i), t)
    ys = lambda i: (lax.bitwise_xor(kv, i), t)
    ts = lambda i: (kv, lax.bitwise_xor(t, i))

    far = z != t
    rows_to = lambda i: (8 * t + y, lax.bitwise_xor(t, i))
    rows_of = lambda i: (lax.bitwise_xor(kv, 8 * i), z)

    barrier = pltpu.get_barrier_semaphore()

    def greet(who):
        pl.semaphore_signal(barrier, inc=1, device_id=who, device_id_type=MESH)

    @pl.when(far)
    def _():
        greet(rows_to(0))
        greet(rows_of(0))

    for i in T_FAR_FIRST:
        greet(rows_to(i))
    for who in (rows_of, zs, ys):
        for i in RING_FAR_FIRST:
            greet(who(i))

    loads = []

    def load(src, dst):
        c = pltpu.make_async_copy(src, dst, lsem.at[len(loads)])
        c.start()
        loads.append(c)
        return c

    l_tok = load(tok_h, tok)
    l_gmix = load(gmix_h, gmix)
    l_wi = load(wi_h, wi)
    l_wf = load(wf_h, wf)
    l_gm = load(gm_h, gm)
    l_w1 = load(wq_h, w1g.at[z])
    l_wk = load(wk_h, w2g.at[z, :, pl.ds(0, 256)])
    l_wv = load(wv_h, w2g.at[z, :, pl.ds(256, 256)])
    l_wm = load(wm_h, wmg.at[z])
    l_wu = load(wu_h, wug.at[z])
    own_units = pl.ds(pl.multiple_of(128 * y, 128), 128)
    l_wd = load(wd_h, wdo)
    l_wdy = load(wd_h.at[:, own_units], wdg.at[z, y])
    cell = [
        load(a, b)
        for a, b in (
            (st_h, st), (smax_h, smax), (k_h, kb), (v_h, vb), (ig_h, igb), (fg_h, fgb), (len_h, lens), (gh_h, gh),
            (bi_h, bi), (bf_h, bfg),
        )
    ]

    pending, arrived = [], set()

    def send(n, src, buf, slot, who):
        dst = buf.at[slot]
        for i in T_FAR_FIRST if who is ts else RING_FAR_FIRST:
            c = pltpu.make_async_remote_copy(
                src_ref=src(i), dst_ref=dst, send_sem=ssem.at[n], recv_sem=rsem.at[n], device_id=who(i), device_id_type=MESH
            )
            c.start()
        pending.append((n, buf))

    def arrive(n, buf):
        arrived.add(n)
        part = buf.at[pl.ds(0, 7)]
        pltpu.make_async_copy(part, part, rsem.at[n]).wait()

    def left(n, buf):
        part = buf.at[pl.ds(0, 7)]
        pltpu.make_async_copy(part, part, ssem.at[n]).wait()

    def start_one(n, src, dst, who):
        pltpu.make_async_remote_copy(
            src_ref=src, dst_ref=dst, send_sem=ssem.at[n], recv_sem=rsem.at[n], device_id=who, device_id_type=MESH
        ).start()

    def send_cross(n, src, buf, slot, who):
        for i in T_FAR_FIRST if who is rows_to else RING_FAR_FIRST:
            start_one(n, src(i), buf.at[slot], who(i))

        @pl.when(far)
        def _():
            start_one(n, src(0), buf.at[slot], who(0))

        @pl.when(z == t)
        def _():
            buf[slot] = src(0)[...]

    zn = lambda k: lax.bitwise_and(z + k, 7)
    on_z = lambda k: (8 * zn(k) + y, t)

    def relay_copy(n, chunk, who, sem):
        pltpu.make_async_remote_copy(
            src_ref=chunk, dst_ref=chunk, send_sem=ssem.at[n], recv_sem=rsem.at[sem], device_id=who, device_id_type=MESH
        ).start()

    def spread(n, buf, ks=(2, -2, 1, -1)):
        for k in ks:
            relay_copy(n, buf.at[z], on_z(k), n if abs(k) == 2 else 24 + n)
        if n not in arrived:
            pending.append((n, buf))
        arrived.add(n)

    def relay(n, buf):
        part = buf.at[pl.ds(0, 2)]
        pltpu.make_async_copy(part, part, rsem.at[n]).wait()
        half = buf.shape[2] // 2
        relay_copy(n, buf.at[zn(-2), :, pl.ds(0, half)], on_z(2), 48 + n)
        relay_copy(n, buf.at[zn(2), :, pl.ds(half, half)], on_z(-2), 48 + n)
        relay_copy(n, buf.at[zn(-2)], on_z(1), 48 + n)
        relay_copy(n, buf.at[zn(2)], on_z(-1), 48 + n)

    def collected(n, buf):
        part = buf.at[pl.ds(0, 2)]
        pltpu.make_async_copy(part, part, rsem.at[24 + n]).wait()
        part = buf.at[pl.ds(0, 3)]
        pltpu.make_async_copy(part, part, rsem.at[48 + n]).wait()

    def cross_done(sem, buf):
        @pl.when(far)
        def _():
            pltpu.make_async_copy(buf, buf, sem).wait()

        @pl.when(z == t)
        def _():
            part = buf.at[pl.ds(0, buf.shape[0] - 1)]
            pltpu.make_async_copy(part, part, sem).wait()

    l_tok.wait()
    placed = jnp.dot(
        tok[...], at_lanes(32, 32 * lax.bitwise_and(z, 1), 128).astype(BF16), preferred_element_type=F32
    )
    ma[...] = (placed[0:16] + pltpu.roll(placed[16:32], 64, 1)).astype(BF16)
    pl.semaphore_wait(barrier, 30 - 2 * (z == t).astype(jnp.int32))
    send_cross(0, lambda i: ma, ra, z, rows_to)

    l_wi.wait()
    l_wf.wait()
    l_gm.wait()
    l_gmix.wait()

    def parts(g):
        first = g.astype(BF16).astype(F32)
        second = (g - first).astype(BF16).astype(F32)
        return first, second, g - first - second

    place = at_lanes(32, 32 * lax.bitwise_and(z, 3), 128).astype(BF16)
    row8 = lax.broadcasted_iota(jnp.int32, (8, 32), 0)
    eight = jnp.zeros((8, 32), F32)
    for r, v in enumerate((wi[...].astype(F32), wf[...].astype(F32), *parts(gm[...]), *parts(gmix[...]))):
        eight = jnp.where(row8 == r, jnp.broadcast_to(v, (8, 32)), eight)
    a2[z] = jnp.dot(eight.astype(BF16), place, preferred_element_type=F32).astype(BF16)
    l_w1.wait()
    spread(2, w1g, (2, -2))
    l_wk.wait()
    l_wv.wait()
    spread(3, w2g, (2, -2))
    spread(2, w1g, (1, -1))
    send(1, lambda i: a2.at[z], a2, z, zs)
    spread(3, w2g, (1, -1))
    l_wd.wait()

    def units(i):
        return wdo.at[:, pl.ds(pl.multiple_of(128 * lax.bitwise_xor(y, i), 128), 128)]

    send(16, units, wdg.at[z], y, ys)

    for c in cell:
        c.wait()
    rows8[...] = jnp.zeros(rows8.shape, F32)
    for s in range(4):
        rows8[0, s : s + 1, :] = igb[s]
        rows8[1, s : s + 1, :] = fgb[s]
    lane = lax.broadcasted_iota(jnp.int32, (8, 128), 1)
    row = lax.broadcasted_iota(jnp.int32, (8, 128), 0)
    live = lane.astype(F32) < column(lens, 8)
    forget_live = jnp.where(live, rows8[1], 0.0)
    total = jnp.sum(forget_live, axis=1, keepdims=True)
    after = jnp.where(
        lax.broadcasted_iota(jnp.int32, (128, 128), 0) > lax.broadcasted_iota(jnp.int32, (128, 128), 1), 1.0, 0.0
    )
    past0 = rows8[0] + jnp.dot(forget_live, after, precision=lax.Precision.HIGHEST, preferred_element_type=F32)
    past0_top = jnp.max(jnp.where(live, past0, -1e30), axis=1, keepdims=True)
    carried0 = column(smax, 8) + total
    q16[...] = jnp.zeros(q16.shape, F32)
    w16[...] = jnp.zeros(w16.shape, F32)

    relay(2, w1g)
    relay(3, w2g)
    l_wm.wait()
    spread(5, wmg)
    cross_done(rsem.at[0], ra)
    low = lax.broadcasted_iota(jnp.int32, (16, 128), 1) < 64
    for h in range(2):
        one = ra[4 * h].astype(F32) + ra[4 * h + 1].astype(F32)
        two = ra[4 * h + 2].astype(F32) + ra[4 * h + 3].astype(F32)
        xraw[0:16, 128 * h : 128 * h + 128] = jnp.where(low, one, pltpu.roll(two, 64, 1))
        xraw[16:32, 128 * h : 128 * h + 128] = jnp.where(low, pltpu.roll(one, 64, 1), two)
    xr = xraw[...]
    square_in = jnp.sum(xr * xr, axis=1, keepdims=True)
    arrive(1, a2)
    halves = []
    for h in range(2):
        half = a2[4 * h].astype(F32)
        for j in range(1, 4):
            half += a2[4 * h + j].astype(F32)
        halves.append(half)
    small = jnp.concatenate(halves, axis=1)
    wgates = jnp.concatenate([small, jnp.zeros((120, 256), F32)], axis=0).astype(BF16)
    gain_mid = small[2:3] + small[3:4] + small[4:5]
    x = (xr * (small[5:6] + small[6:7] + small[7:8])).astype(BF16)
    lane32 = lax.broadcasted_iota(jnp.int32, (32, 128), 1)

    def with_square(block, sq, at):
        hi = sq.astype(BF16).astype(F32)
        return jnp.where(lane32 == at, hi, jnp.where(lane32 == at + 1, sq - hi, block))

    gates = with_square(contract_last(x, wgates), square_in, 2)
    collected(2, w1g)
    q_part = jnp.dot(x, w1g[...].reshape(256, 256), preferred_element_type=F32)
    for j in range(8):
        mz1[j, :, 0:256] = q_part[4 * j : 4 * j + 4].astype(BF16)
        mz1[j, :, 256:384] = gates[4 * j : 4 * j + 4].astype(BF16)
    send(6, lambda i: mz1.at[lax.bitwise_xor(y, i)], rz1, y, ys)
    rz1[y] = mz1[y]
    l_wu.wait()
    spread(7, wug)
    collected(3, w2g)
    kv_part = jnp.dot(x, w2g[...].reshape(256, 512), preferred_element_type=F32)
    for j in range(8):
        mz2[j] = kv_part[4 * j : 4 * j + 4].astype(BF16)
    rz2[y] = mz2[y]
    send(8, lambda i: mz2.at[lax.bitwise_xor(y, i)], rz2, y, ys)
    relay(5, wmg)
    l_wdy.wait()
    arrive(16, wdg.at[z])
    spread(9, wdg)

    for s in range(4):
        hi = st[s, 0].astype(BF16)
        shi[s] = hi
        slo[s] = (st[s, 0] - hi.astype(F32)).astype(BF16)
    arrive(6, rz1)
    first = rz1[0].astype(F32)
    for j in range(1, 8):
        first += rz1[j].astype(F32)
    own = first[:, 256:384]
    factor = lax.rsqrt((own[:, 2:3] + own[:, 3:4]) / D + EPS)
    q16[0:4, :] = first[:, 0:256] * factor
    rows8[2, 0:4, :] = own * factor
    gate8 = rows8[2]
    input_gate = gate8[:, 0:1] + bi[...]
    pre = gate8[:, 1:2] + bfg[...]
    forget_gate = jnp.minimum(pre, 0.0) - jnp.log1p(jnp.exp(-jnp.abs(pre)))
    carried = carried0 + forget_gate
    topmost = jnp.maximum(jnp.maximum(carried, input_gate), past0_top + forget_gate)
    decay = jnp.where(live, jnp.exp(jnp.minimum(past0 + forget_gate - topmost, 0.0)), 0.0)
    qb = q16[...].astype(BF16)
    scores = jnp.zeros((8, 128), F32)
    state = jnp.zeros((8, 256), F32)
    row256 = lax.broadcasted_iota(jnp.int32, (8, 256), 0)
    for s in range(4):
        scores = jnp.where(row == s, contract_last(qb, kb[s, 0])[0:8], scores)
        part = contract_last(qb, shi[s])[0:8] + contract_last(qb, slo[s])[0:8]
        state = jnp.where(row256 == s, part, state)
    w16[0:8, :] = decay * (scores * SCALE)
    wb = w16[...].astype(BF16)
    block = jnp.zeros((8, 256), F32)
    for s in range(4):
        block = jnp.where(row256 == s, jnp.dot(wb, vb[s, 0], preferred_element_type=F32)[0:8], block)
    numerator = jnp.exp(carried - topmost) * state + block
    own_scale = jnp.exp(input_gate - topmost) * SCALE

    arrive(8, rz2)
    second = rz2[0].astype(F32)
    for j in range(1, 8):
        second += rz2[j].astype(F32)
    second = (second * factor).astype(BF16).astype(F32)
    own_score = jnp.sum(qb[0:4].astype(F32) * second[:, 0:256], axis=1, keepdims=True)
    num = numerator[0:4] + (own_scale[0:4] * own_score) * second[:, 256:512]
    mixed = num * lax.rsqrt(jnp.mean(num * num, axis=1, keepdims=True) + EPS) * gh[...]
    mc[...] = mixed.astype(BF16)
    send(10, lambda i: mc, rc, y, ys)
    rc[y] = mixed.astype(BF16)
    relay(7, wug)

    collected(5, wmg)
    arrive(10, rc)
    for j in range(8):
        m32[4 * j : 4 * j + 4, :] = rc[j].astype(F32)
    att = contract_last(m32[...].astype(BF16), wmg[...].reshape(256, 256)).astype(BF16)
    md[...] = att
    send(11, lambda i: md, rd, t, ts)
    rd[t] = att
    relay(9, wdg)
    arrive(11, rd)
    attended = rd[0].astype(F32)
    for j in range(1, 8):
        attended += rd[j].astype(F32)
    restored = (xraw[...] + attended).astype(BF16).astype(F32)

    square_mid = jnp.sum(restored * restored, axis=1, keepdims=True)
    tile = lax.broadcasted_iota(jnp.int32, (8, 128), 1)
    high = square_mid.astype(BF16).astype(F32)
    sq_rows = jnp.zeros((8, 128), F32)
    for g in range(4):
        sq_rows = jnp.where(tile == g, high[8 * g : 8 * g + 8], sq_rows)
        sq_rows = jnp.where(tile == 4 + g, (square_mid - high)[8 * g : 8 * g + 8], sq_rows)
    sq_rows = jnp.concatenate([sq_rows, jnp.zeros((8, 128), F32)], axis=0).astype(BF16)
    collected(7, wug)
    up = jnp.dot((restored * gain_mid).astype(BF16), wug[...].reshape(256, 1024), preferred_element_type=F32)
    for j in range(8):
        mf[j, 0:32, :] = up[:, 128 * j : 128 * j + 128].astype(BF16)
        mf[j, 32:48, :] = sq_rows
    send(12, lambda i: mf.at[lax.bitwise_xor(y, i)], rf, y, ys)
    rf[y] = mf[y]
    sent = contract_last(restored.astype(BF16), at_lanes(32, 32 * t, 256).astype(BF16)).astype(BF16)
    mp[...] = sent

    @pl.when(far)
    def _():
        start_one(14, mp, rp, rows_to(lax.bitwise_xor(z, t)))

    @pl.when(z == t)
    def _():
        rp[...] = mp[...]
    arrive(12, rf)
    whole = rf[0].astype(F32)
    for j in range(1, 8):
        whole += rf[j].astype(F32)
    squares = jnp.concatenate(
        [whole[32:40, g : g + 1] + whole[32:40, 4 + g : 5 + g] for g in range(4)], axis=0
    )
    factor_mid = lax.rsqrt(squares / D + EPS)
    hid = jnp.square(jnp.maximum(whole[0:32] * factor_mid, 0.0)).astype(BF16)

    group = lax.shift_right_logical(tile, 5)
    collected(9, wdg)
    for jj in (*RING_FAR_FIRST, 0):
        zz = lax.bitwise_xor(z, jj)
        down = contract_last(hid, wdg[zz].reshape(256, 128))
        for h in range(2):
            part = down[:, 128 * h : 128 * h + 128]
            turned = [part] + [pltpu.roll(part, 32 * k, 1) for k in range(1, 4)]
            for d in range(4):
                packed = jnp.zeros((8, 128), F32)
                for g in range(4):
                    packed = jnp.where(group == g, turned[(g - d) % 4][8 * g : 8 * g + 8], packed)
                mh[8 * jj + 4 * h + d] = packed.astype(BF16)
        for i in (*RING_FAR_FIRST, 0) if jj else RING_FAR_FIRST:
            yy = lax.bitwise_xor(y, i)
            start_one(15, mh.at[8 * jj + yy], rh.at[8 * t + y], (8 * zz + yy, z))

    @pl.when(far)
    def _():
        start_one(15, mh.at[y], rh.at[8 * t + y], (kv, z))

    @pl.when(z == t)
    def _():
        rh[8 * t + y] = mh[y]

    @pl.when(far)
    def _():
        pltpu.make_async_copy(rp, rp, rsem.at[14]).wait()

    cross_done(rsem.at[15], rh)
    summed = rh[0].astype(F32)
    for j in range(1, 64):
        summed += rh[j].astype(F32)
    for g in range(4):
        rows = slice(8 * g, 8 * g + 8)
        out_ref[rows, :] = rp[rows, :].astype(F32) + summed[:, 32 * g : 32 * g + 32]

    for n, buf in pending:
        left(n, buf)
    cross_done(ssem.at[0], ra)
    cross_done(ssem.at[15], rh)

    @pl.when(far)
    def _():
        pltpu.make_async_copy(mp, mp, ssem.at[14]).wait()


def body(
    tokens, gain_mix, w_query, w_key, w_value, w_igate, w_fgate, bias_igate, bias_fgate, state_mem, state_max, keys_blk,
    values_blk, igate_blk, fgate_blk, lengths, gain_head, w_mixout, gain_mlp, w_up, w_down,
):
    args = (
        tokens, gain_mix.reshape(1, 32), w_query, w_key, w_value, w_igate.T, w_fgate.T, bias_igate.reshape(1, 1),
        bias_fgate.reshape(1, 1), state_mem, state_max.T, keys_blk, values_blk, igate_blk, fgate_blk, lengths.reshape(1, 4),
        gain_head.reshape(1, 256), w_mixout.T, gain_mlp.reshape(1, 32), w_up, w_down.T,
    )
    vm = pltpu.VMEM
    out = pl.pallas_call(
        kernel,
        out_shape=pltpu.VMEM((32, 32), F32),
        in_specs=[pl.BlockSpec(memory_space=pl.ANY)] * 21,
        out_specs=pl.BlockSpec(memory_space=pltpu.VMEM),
        scratch_shapes=[
            vm((32, 32), BF16), vm((1, 32), F32), vm((1, 32), BF16), vm((1, 32), BF16), vm((1, 1), F32), vm((1, 1), F32),
            vm((4, 1, 256, 256), F32), vm((1, 4), F32), vm((4, 1, 128, 256), BF16), vm((4, 1, 128, 256), BF16),
            vm((4, 1, 128), F32), vm((4, 1, 128), F32), vm((1, 4), jnp.int32), vm((1, 256), F32), vm((1, 32), F32),
            vm((8, 32, 256), BF16), vm((8, 32, 512), BF16), vm((8, 32, 256), BF16), vm((8, 32, 1024), BF16),
            vm((32, 1024), BF16), vm((8, 8, 32, 128), BF16),
            vm((16, 128), BF16), vm((8, 16, 128), BF16), vm((8, 8, 128), BF16), vm((32, 256), F32), vm((8, 4, 384), BF16), vm((8, 4, 384), BF16), vm((8, 4, 512), BF16),
            vm((8, 4, 512), BF16), vm((4, 256, 256), BF16), vm((4, 256, 256), BF16), vm((3, 8, 128), F32), vm((16, 256), F32),
            vm((16, 128), F32), vm((4, 256), BF16), vm((8, 4, 256), BF16), vm((32, 256), F32), vm((32, 256), BF16),
            vm((8, 32, 256), BF16), vm((8, 48, 128), BF16), vm((8, 48, 128), BF16),
            vm((64, 8, 128), BF16), vm((64, 8, 128), BF16), vm((32, 32), BF16),
            vm((32, 32), BF16),
            pltpu.SemaphoreType.DMA((22,)), pltpu.SemaphoreType.DMA((24,)), pltpu.SemaphoreType.DMA((72,)),
        ],
        compiler_params=pltpu.CompilerParams(collective_id=0, has_side_effects=True),
    )(*args)
    return out.astype(BF16)


def solution(mesh):
    in_specs = (
        P("tp", "kv"),
        P("kv"),
        P("kv", "tp"),
        P("kv", "tp"),
        P("kv", "tp"),
        P("kv", "tp"),
        P("kv", "tp"),
        P("tp"),
        P("tp"),
        P("kv", "tp", None, None),
        P("kv", "tp"),
        P("kv", "tp", None, None),
        P("kv", "tp", None, None),
        P("kv", "tp", None),
        P("kv", "tp", None),
        P("kv"),
        P(),
        P("tp", "kv"),
        P("kv"),
        P("kv", "tp"),
        P("tp", "kv"),
    )
    return jax.shard_map(body, mesh=mesh, in_specs=in_specs, out_specs=P("tp", "kv"), check_vma=False)
```
